32 devices in a mesh: fs: 8 (over z, y), tp: 4 (over x, core).
Axes of the slice: x: 2, y: 2, z: 4, core: 2. Of those that a mesh axis runs over, the one named last changes fastest.
Arguments:
- tokens: bfloat16 [4096, 2048], P(('fs', 'tp')), may hold values from -6 to 6
- gate_proj: bfloat16 [2048, 512], P('fs', 'tp'), may hold values from -0.125 to 0.125
- signal_proj: bfloat16 [2048, 512], P('fs', 'tp'), may hold values from -1.5467961 to 1.5467961
- spatial: bfloat16 [4, 128, 128], replicated, may hold values from -0.5 to 0.5
- signal_gain: bfloat16 [512], P('tp'), may hold values from 0.099609375 to 1.8984375
- mixer_out: bfloat16 [512, 2048], P('tp', 'fs'), may hold values from -0.25 to 0.25
- mixer_gain: bfloat16 [2048], replicated, may hold values from 0.099609375 to 1.8984375
- ffn_gate: bfloat16 [2048, 5632], P('fs', 'tp'), may hold values from -0.125 to 0.125
- ffn_value: bfloat16 [2048, 5632], P('fs', 'tp'), may hold values from -0.125 to 0.125
- conv_taps: bfloat16 [3, 5632], P(None, 'tp'), may hold values from -3.5 to 3.5
- ffn_down: bfloat16 [5632, 2048], P('tp', 'fs'), may hold values from -0.078125 to 0.078125
- output_gain: bfloat16 [2048], replicated, may hold values from 0.099609375 to 1.8984375
Outputs:
- result: bfloat16 [4096, 2048], P(('fs', 'tp'))
The draws below stay inside these ranges and needn't reach their ends.
All inputs are finite; a program needn't handle non-finite values.
Results may differ from the reference program's by a relative error of at most 0.01.
Values may be sent and summed in bfloat16 or wider, within the bound.
A program may use at most 64 MiB of HBM per device.

```python
import math
import jax
import jax.numpy as jnp
from jax import lax

D = 2048
MIX_WIDTH = 512
HEAD_SIZE = 128
HEADS = 4
BLOCK = 128
SEGMENT = 64
FF = 5632
SEQ = 512
TOKENS = 4096
N_FS = 8
N_TP = 4


def draw_signal_proj(key, part):
    first_key, second_key = jax.random.split(jax.random.fold_in(key, 17))
    column = jnp.arange(MIX_WIDTH, dtype=jnp.float32) / MIX_WIDTH
    jitter = jnp.exp(jax.random.uniform(second_key, (MIX_WIDTH,), jnp.float32, -0.35, 0.35))
    entries = jnp.clip(jax.random.normal(first_key, (D, MIX_WIDTH), jnp.float32), -6.0, 6.0)
    rising = 4.0 ** column
    scales = rising * jitter / jnp.sqrt(jnp.float32(D))
    return (entries * scales[None, :]).astype(jnp.bfloat16)


def levels(stream_key, dims, cuts, low, top_value):
    def one(axis_at, blocks):
        draws = jax.random.uniform(jax.random.fold_in(jax.random.fold_in(stream_key, 6), axis_at), (blocks,), jnp.float32, low / len(cuts), top_value / len(cuts))
        return jnp.repeat(jnp.exp(draws), dims[axis_at] // blocks).reshape((-1,) + (1,) * (len(dims) - axis_at - 1))

    factor_of = one(*cuts[0])
    for cut in cuts[1:]:
        factor_of = factor_of * one(*cut)
    return factor_of


def scatter_about(key, dims, scale, most, cuts=(), kind=jnp.bfloat16):
    drawn = scale * jax.random.normal(key, dims, jnp.float32)
    if cuts:
        drawn = drawn * levels(key, dims, cuts, -0.22, 0.18)
    return jnp.clip(drawn, -most, most).astype(kind)


def setup_inputs(seed: int = 0) -> dict:
    seeds = jax.random.split(jax.random.key(seed), 13)
    return {
        "tokens": scatter_about(seeds[0], (TOKENS, D), 1.0, 6.0, ((0, 32),)),
        "gate_proj": scatter_about(seeds[1], (D, MIX_WIDTH), D ** -0.5, 0.125, ((0, 8), (1, 4))),
        "signal_proj": draw_signal_proj(jax.random.fold_in(seeds[12], 71), 0),
        "spatial": scatter_about(seeds[3], (HEADS, BLOCK, BLOCK), BLOCK ** -0.5, 0.5),
        "signal_gain": jnp.clip(1.0 + 0.18 * jax.random.normal(seeds[4], (MIX_WIDTH,), jnp.float32), 0.099609375, 1.8984375).astype(jnp.bfloat16),
        "mixer_out": scatter_about(seeds[5], (MIX_WIDTH, D), MIX_WIDTH ** -0.5, 0.25, ((0, 4), (1, 8))),
        "mixer_gain": jnp.clip(1.0 + 0.18 * jax.random.normal(seeds[6], (D,), jnp.float32), 0.099609375, 1.8984375).astype(jnp.bfloat16),
        "ffn_gate": scatter_about(seeds[7], (D, FF), D ** -0.5, 0.125, ((0, 8), (1, 4))),
        "ffn_value": scatter_about(seeds[8], (D, FF), D ** -0.5, 0.125, ((0, 8), (1, 4))),
        "conv_taps": scatter_about(seeds[9], (3, FF), 3 ** -0.5, 3.5, ((1, 4),)),
        "ffn_down": scatter_about(seeds[10], (FF, D), FF ** -0.5, 0.078125, ((0, 4), (1, 8))),
        "output_gain": jnp.clip(1.0 + 0.18 * jax.random.normal(seeds[11], (D,), jnp.float32), 0.099609375, 1.8984375).astype(jnp.bfloat16),
    }


EPSILON = 1e-05
RESIDUAL_SCALE = math.sqrt(2.0)

def normalize(values):
    row_mean = lax.optimization_barrier(jnp.mean(values, axis=-1, keepdims=True))
    centred = values - row_mean
    spread = lax.optimization_barrier(jnp.mean(centred * centred, axis=-1, keepdims=True))
    return centred * lax.rsqrt(spread + EPSILON)

def one_sequence(sequence, gate_proj, signal_proj, spatial, signal_gain, mixer_out, mixer_gain, ffn_gate, ffn_value, conv_taps, ffn_down, output_gain):
    residual = sequence.astype(jnp.float32)
    mix_input = normalize(residual).astype(jnp.bfloat16)
    branch_gate = jax.nn.gelu(jnp.dot(mix_input, gate_proj, preferred_element_type=jnp.float32))
    branch_signal = jax.nn.gelu(jnp.dot(mix_input, signal_proj, preferred_element_type=jnp.float32))
    spatial_input = (normalize(branch_signal) * signal_gain.astype(jnp.float32)).astype(jnp.bfloat16)
    segment_ids = jnp.arange(BLOCK) // SEGMENT
    allowed = segment_ids[None, :] <= segment_ids[:, None]
    masked = jnp.where(allowed[None], spatial, jnp.zeros_like(spatial))
    blocks = spatial_input.reshape(SEQ // BLOCK, BLOCK, HEADS, HEAD_SIZE)
    mixed = jnp.einsum('hij,njhd->nihd', masked.astype(jnp.float32), blocks.astype(jnp.float32)).reshape(SEQ, MIX_WIDTH)
    gated = (branch_gate * mixed).astype(jnp.bfloat16)
    mix_out = jnp.dot(gated, mixer_out, preferred_element_type=jnp.float32)
    middle = (normalize(RESIDUAL_SCALE * residual + mix_out) * mixer_gain.astype(jnp.float32)).astype(jnp.bfloat16)
    middle_wide = middle.astype(jnp.float32)
    ffn_input = normalize(middle_wide).astype(jnp.bfloat16)
    gate_pre = jnp.dot(ffn_input, ffn_gate, preferred_element_type=jnp.float32)
    value_pre = jnp.dot(ffn_input, ffn_value, preferred_element_type=jnp.float32)
    taps = conv_taps.astype(jnp.float32)
    shifted_one = jnp.concatenate([jnp.zeros((1, FF), jnp.float32), gate_pre[:-1]], axis=0)
    shifted_two = jnp.concatenate([jnp.zeros((2, FF), jnp.float32), gate_pre[:-2]], axis=0)
    conv_gate = taps[0] * shifted_two + taps[1] * shifted_one + taps[2] * gate_pre
    hidden = (jax.nn.silu(conv_gate) * value_pre).astype(jnp.bfloat16)
    group_width = FF // N_TP
    ffn_out = jnp.zeros((SEQ, D), jnp.float32)
    for group in range(N_TP):
        partial_sum = jnp.dot(hidden[:, group * group_width:(group + 1) * group_width], ffn_down[group * group_width:(group + 1) * group_width], preferred_element_type=jnp.float32)
        rounded = lax.optimization_barrier(partial_sum.astype(jnp.bfloat16))
        ffn_out = ffn_out + rounded.astype(jnp.float32)
    return (normalize(RESIDUAL_SCALE * middle_wide + ffn_out) * output_gain.astype(jnp.float32)).astype(jnp.bfloat16)

def reference(tokens, gate_proj, signal_proj, spatial, signal_gain, mixer_out, mixer_gain, ffn_gate, ffn_value, conv_taps, ffn_down, output_gain):
    sequences = tokens.reshape(N_FS, SEQ, D)

    def apply_layer(sequence):
        return one_sequence(sequence, gate_proj, signal_proj, spatial, signal_gain, mixer_out, mixer_gain, ffn_gate, ffn_value, conv_taps, ffn_down, output_gain)
    outputs = lax.map(apply_layer, sequences)
    return outputs.reshape(TOKENS, D)
```

```python
import functools
import math

import jax
import jax.numpy as jnp
from jax import lax
from jax.experimental import pallas as pl
from jax.experimental.pallas import tpu as pltpu
from jax.sharding import PartitionSpec as P

MIX_WIDTH = 512
HEAD_SIZE = 128
BLOCK = 128
SEGMENT = 64
LANES = 128
GV_PIECES = 4
DN_PIECES = 2
EARLY = 2
EPSILON = 1e-05
RESIDUAL_SCALE = math.sqrt(2.0)
MESH = pl.DeviceIdType.MESH
F32 = jnp.float32
BF16 = jnp.bfloat16


def normalize(values):
    row_mean = jnp.mean(values, axis=-1, keepdims=True)
    centred = values - row_mean
    spread = jnp.mean(centred * centred, axis=-1, keepdims=True)
    return centred * lax.rsqrt(spread + EPSILON)


def kernel(
    nz, ny, nx, full, rem, subs, packed,
    tok, gp, sp_, mo, fg, fv, gt, vt, dn, spatial, sgain, mgain, taps, ogain,
    out,
    gsb, mob, gvb, dnb, tails, mixed, xin, stat, pm, prc, abm, pxr, mid, hin, hid, pb, rb, ab, xr, zb, zr,
    loc_sem, gzs, gzr, gys, gyr, mzs, mzr, mys, myr, zs, zrs, ys, yrs, ts, trs,
):
    R, D = tok.shape
    C, cw = mo.shape
    K = fg.shape[0]
    F = full
    W = full + rem
    MW = mixed.shape[2]
    f = lax.axis_index("fs")
    t = lax.axis_index("tp")
    z, y = f // ny, f % ny
    x, c = t // 2, t % 2
    q = z % 2
    seq = nx * 2 * R
    gw = ny * cw

    def zsrc(d):
        zz = z
        for bit in (1 << k for k in range(d.bit_length())):
            if d & bit:
                zz = zz + bit - 2 * bit * ((z // bit) % 2)
        return zz

    def zpeer(d):
        return (zsrc(d) * ny + y, t)

    def ypeer(e):
        return (z * ny + lax.rem(y + e, ny), t)

    def xpeer(d):
        return (f, lax.rem(x + d, nx) * 2 + c)

    def tpeer(d, e):
        return (f, lax.rem(x + d, nx) * 2 + (c if e == 0 else 1 - c))

    cpeer = (f, x * 2 + 1 - c)
    ppeer = ((z + 1 - 2 * q) * ny + y, t)

    def ysrc(e):
        return lax.rem(y + ny - e, ny)

    def xsrc(d):
        return lax.rem(x + nx - d, nx)

    pending = []

    def remote(src, dst, ssem, rsem, to):
        return pltpu.make_async_remote_copy(
            src_ref=src, dst_ref=dst, send_sem=ssem, recv_sem=rsem, device_id=to, device_id_type=MESH
        )

    def when(cond, action):
        if cond is None:
            action()
        else:
            pl.when(cond)(action)

    def send(src, dst, ssem, rsem, to, cond=None):
        copy = remote(src, dst, ssem, rsem, to)
        when(cond, lambda: copy.start())
        pending.append((copy, cond))

    def arrived(dst, ssem, rsem, to):
        remote(dst, dst, ssem, rsem, to).wait_recv()

    scope = jax.named_scope
    tslot = [0]

    def tsem():
        k = tslot[0]
        tslot[0] += 1
        return ts.at[k], trs.at[k]

    gv_rows = K // GV_PIECES
    dn_rows = W // DN_PIECES
    DN = GV_PIECES

    def parts(a, h, zz, yy):
        if a < DN:
            rows = pl.ds(a * gv_rows, gv_rows)
            dst = gvb.at[zz, yy]
            at = pl.multiple_of(h * F, LANES)
            return [
                (fg.at[rows, pl.ds(at, F)], dst.at[rows, pl.ds(0, F)]),
                (fv.at[rows, pl.ds(at, F)], dst.at[rows, pl.ds(F, F)]),
                (mixed.at[h, rows], dst.at[rows, pl.ds(2 * F, MW)]),
            ]
        lo, hi = (a - DN) * dn_rows, (a - DN + 1) * dn_rows
        dst = dnb.at[zz, yy]
        found = []
        if lo < F:
            n = min(hi, F) - lo
            found.append((dn.at[pl.ds(pl.multiple_of(h * F + lo, 16), n)], dst.at[pl.ds(lo, n)]))
        if hi > F:
            s = max(lo, F)
            n = hi - s
            found.append(
                (dn.at[pl.ds(pl.multiple_of(2 * F + h * rem + s - F, 16), n)], dst.at[pl.ds(s, n)])
            )
        return found

    def slot(a, zz, yy):
        if a < DN:
            return gvb.at[zz, yy, pl.ds(a * gv_rows, gv_rows)]
        return dnb.at[zz, yy, pl.ds((a - DN) * dn_rows, dn_rows)]

    lk = [0]
    held = {}

    def fetch(key, src, dst):
        copy = pltpu.make_async_copy(src, dst, loc_sem.at[lk[0]])
        lk[0] += 1
        copy.start()
        held.setdefault(key, []).append(copy)

    def ready(key):
        for copy in held.pop(key):
            copy.wait()

    if packed:
        fetch("gs", gp, gsb.at[z, y])
    else:
        fetch("gs", gp, gsb.at[z, y, :, pl.ds(0, C)])
        fetch("gs", sp_, gsb.at[z, y, :, pl.ds(C, C)])
    fetch("mo", mo, mob.at[z, y])
    T = tails.shape[2]
    if packed:
        fetch("tails", gt, tails.at[0])
        fetch("tails", vt, tails.at[1])
    else:
        fetch("tails", gt.at[:, pl.ds(2 * F, T)], tails.at[0])
        fetch("tails", vt.at[:, pl.ds(2 * F, T)], tails.at[1])
    for a in range(DN):
        for src, dst in parts(a, q, z, y)[:2]:
            fetch("gv", src, dst)
    for a in range(DN, DN + DN_PIECES):
        for src, dst in parts(a, q, z, y):
            fetch("dn", src, dst)

    barrier = pltpu.get_barrier_semaphore()
    peers = [zpeer(d) for d in range(1, nz)] + [ypeer(e) for e in range(1, ny)]
    peers += [tpeer(d, e) for d in range(nx) for e in range(2) if d + e]
    for p in peers:
        pl.semaphore_signal(barrier, inc=1, device_id=p, device_id_type=MESH)

    ready("tails")
    for h in range(2):
        for k in range(2):
            mixed[h, :, k * (MW // 2):k * (MW // 2) + rem] = tails[k, :, h * rem:(h + 1) * rem]
    for k in range(2):
        part = tails[k].astype(F32)
        part = jnp.where(q == 0, part[:, :rem], part[:, rem:2 * rem]).astype(BF16)
        gvb[z, y, :, 2 * F + k * (MW // 2):2 * F + k * (MW // 2) + rem] = part
    ready("gs")
    ready("mo")
    pl.semaphore_wait(barrier, len(peers))

    def issue_z(a, d):
        for src, dst in parts(a, zsrc(d) % 2, z, y):
            remote(src, dst, zs.at[a, d], zrs.at[a, d], zpeer(d)).start()
        whole = slot(a, z, y)
        pending.append((remote(whole, whole, zs.at[a, d], zrs.at[a, d], zpeer(d)), None))

    def issue_all(a):
        for d in range(1, nz):
            issue_z(a, d)

    def issue_y(a):
        for e in range(1, ny):
            send(slot(a, z, y), slot(a, z, y), ys.at[a, 0, e], yrs.at[a, 0, e], ypeer(e))

    def relay(a, d):
        zz = zsrc(d)
        arrived(slot(a, zz, y), zs.at[a, d], zrs.at[a, d], zpeer(d))
        for e in range(1, ny):
            send(slot(a, zz, y), slot(a, zz, y), ys.at[a, d, e], yrs.at[a, d, e], ypeer(e))

    def complete(a, d, e):
        zz, yy = zsrc(d), ysrc(e)
        arrived(slot(a, zz, yy), ys.at[a, d, e], yrs.at[a, d, e], ypeer(e))

    own_gs, own_mo = gsb.at[z, y], mob.at[z, y]
    for d in range(1, nz):
        send(own_gs, own_gs, gzs.at[d], gzr.at[d], zpeer(d))
    for d in range(1, nz):
        send(own_mo, own_mo, mzs.at[d], mzr.at[d], zpeer(d))
    for e in range(1, ny):
        send(own_gs, own_gs, gys.at[0, e], gyr.at[0, e], ypeer(e))
    for e in range(1, ny):
        send(own_mo, own_mo, mys.at[0, e], myr.at[0, e], ypeer(e))
    ready("gv")
    issue_y(0)

    xin[x, c] = normalize(tok[...].astype(F32)).astype(BF16)
    s1 = [tsem() for _ in range(nx)]
    s2 = [tsem() for _ in range(nx)]
    for d in range(1, nx):
        send(xin.at[x, c], xin.at[x, c], *s1[d], xpeer(d))
    send(xin.at[x, c], xin.at[x, c], *s2[0], cpeer)

    def pass_on(buf, d, zsem, zrsem, ysem, yrsem):
        block = buf.at[zsrc(d), y]
        arrived(block, zsem.at[d], zrsem.at[d], zpeer(d))
        for e in range(1, ny):
            send(block, block, ysem.at[d, e], yrsem.at[d, e], ypeer(e))

    for d in range(1, nz):
        with scope(f"relay_gs{d}"):
            pass_on(gsb, d, gzs, gzr, gys, gyr)
    for d in range(1, nz):
        with scope(f"relay_mo{d}"):
            pass_on(mob, d, mzs, mzr, mys, myr)
    issue_all(0)
    issue_all(1)
    ready("dn")
    for a in range(1, DN + DN_PIECES):
        issue_y(a)
    with scope("xin"):
        for d in range(1, nx):
            arrived(xin.at[xsrc(d), c], *s1[d], xpeer(d))
            send(xin.at[xsrc(d), c], xin.at[xsrc(d), c], *s2[d], cpeer)
        for d in range(nx):
            arrived(xin.at[xsrc(d), 1 - c], *s2[d], cpeer)
    with scope("complete_gs"):
        for d in range(nz):
            for e in range(1, ny):
                yy = ysrc(e)
                arrived(gsb.at[zsrc(d), yy], gys.at[d, e], gyr.at[d, e], ypeer(e))

    with scope("mix_in"):
        pre = jnp.dot(xin[...].reshape(seq, D), gsb[...].reshape(D, 2 * C), preferred_element_type=F32)
        branch_signal = jax.nn.gelu(pre[:, C:])
        total = jnp.sum(branch_signal, axis=1, keepdims=True)
        square = jnp.sum(branch_signal * branch_signal, axis=1, keepdims=True)
        lane = lax.broadcasted_iota(jnp.int32, (seq, LANES), 1)
        stat[0] = jnp.where(lane == 0, total, square).T[:8]
    others = [(d, e) for d in range(nx) for e in range(2) if d + e]
    sx = {}
    for d, e in others:
        sx[d, e] = tsem()
        send(stat.at[0], stat.at[2 * d + e], *sx[d, e], tpeer(d, e))
    branch_gate = jax.nn.gelu(pre[:, :C])
    with scope("stats"):
        summed = stat[0]
        for d, e in others:
            arrived(stat.at[2 * d + e], *sx[d, e], tpeer(d, e))
            summed = summed + stat[2 * d + e]
    with scope("complete_mo"):
        for d in range(nz):
            for e in range(1, ny):
                arrived(mob.at[zsrc(d), ysrc(e)], mys.at[d, e], myr.at[d, e], ypeer(e))
    with scope("mix_out"):
        back = summed.T
        row_mean = back[:, 0:1] / MIX_WIDTH
        spread = back[:, 1:2] / MIX_WIDTH - row_mean * row_mean
        spatial_input = (
            (branch_signal - row_mean) * lax.rsqrt(spread + EPSILON) * sgain[...].astype(F32)
        ).astype(BF16)
        rows_i = lax.broadcasted_iota(jnp.int32, (BLOCK, BLOCK), 0) // SEGMENT
        cols_i = lax.broadcasted_iota(jnp.int32, (BLOCK, BLOCK), 1) // SEGMENT
        own = spatial[t * C // HEAD_SIZE]
        own = jnp.where(cols_i <= rows_i, own, jnp.zeros_like(own))
        gated = jnp.concatenate(
            [
                branch_gate[b * BLOCK:(b + 1) * BLOCK]
                * jnp.dot(own, spatial_input[b * BLOCK:(b + 1) * BLOCK], preferred_element_type=F32)
                for b in range(seq // BLOCK)
            ],
            axis=0,
        ).astype(BF16)
        for k in range(nz * ny):
            part = jnp.dot(gated, mob[k // ny, k % ny], preferred_element_type=F32).astype(BF16)
            for b in range(nx * 2):
                pm[b % 2, b // 2, :, k * cw:(k + 1) * cw] = part[b * R:(b + 1) * R]
    sc = tsem()
    send(pm.at[1 - c], prc, *sc, cpeer)
    with scope("mix_core"):
        arrived(prc, *sc, cpeer)
    for b in range(nx):
        abm[b] = (pm[c, b].astype(F32) + prc[b].astype(F32)).astype(BF16)
    sx = [tsem() for _ in range(nx)]
    for d in range(1, nx):
        send(abm.at[lax.rem(x + d, nx)], pxr.at[d - 1], *sx[d], xpeer(d))
    with scope("relay_gv0"):
        for d in range(1, nz):
            relay(0, d)
    issue_all(2)
    with scope("mix_x"):
        for d in range(1, nx):
            arrived(pxr.at[d - 1], *sx[d], xpeer(d))
    with scope("mid"):
        mix_out = pm[c, x].astype(F32) + prc[x].astype(F32)
        for d in range(1, nx):
            mix_out = mix_out + pxr[d - 1].astype(F32)
        mid[...] = (
            normalize(RESIDUAL_SCALE * tok[...].astype(F32) + mix_out) * mgain[...].astype(F32)
        ).astype(BF16)
        hin[q, x, c] = normalize(mid[...].astype(F32)).astype(BF16)

    sp = tsem()
    send(hin.at[q, x, c], hin.at[q, x, c], *sp, ppeer)
    sx = [[tsem() for _ in range(nx)] for _ in range(2)]
    sy = [[tsem() for _ in range(nx)] for _ in range(2)]
    for d in range(1, nx):
        send(hin.at[q, x, c], hin.at[q, x, c], *sx[0][d], xpeer(d))
    send(hin.at[q, x, c], hin.at[q, x, c], *sy[0][0], cpeer)
    with scope("relay_gv1"):
        for d in range(1, nz):
            relay(1, d)

    def rows_over(k, s):
        for d in range(1, nx):
            arrived(hin.at[s, xsrc(d), c], *sx[k][d], xpeer(d))
            send(hin.at[s, xsrc(d), c], hin.at[s, xsrc(d), c], *sy[k][d], cpeer)

    with scope("rows_x0"):
        rows_over(0, q)
    for a in range(2, DN):
        with scope(f"relay_gv{a}"):
            for d in range(1, nz):
                relay(a, d)
                if d == 1:
                    issue_all(a + 1)
                elif d == nz - 1 and a == DN - 1:
                    issue_all(a + 2)
        if a == 2:
            with scope("pair_rows"):
                arrived(hin.at[1 - q, x, c], *sp, ppeer)
            for d in range(1, nx):
                send(hin.at[1 - q, x, c], hin.at[1 - q, x, c], *sx[1][d], xpeer(d))
            send(hin.at[1 - q, x, c], hin.at[1 - q, x, c], *sy[1][0], cpeer)
    with scope("rows_x1"):
        rows_over(1, 1 - q)
    with scope("rows_core"):
        for k, s in enumerate((q, 1 - q)):
            for d in range(nx):
                arrived(hin.at[s, xsrc(d), 1 - c], *sy[k][d], cpeer)
    with scope("complete_gv"):
        for a in range(DN):
            for d in range(nz):
                for e in range(1, ny):
                    complete(a, d, e)

    def gate_value(s):
        def finish(gate, value, tap):
            row = lax.broadcasted_iota(jnp.int32, gate.shape, 0)
            one = jnp.where(row >= 1, pltpu.roll(gate, 1, 0), 0.0)
            two = jnp.where(row >= 2, pltpu.roll(gate, 2, 0), 0.0)
            conv = tap[0:1] * two + tap[1:2] * one + tap[2:3] * gate
            return (jax.nn.silu(conv) * value).astype(BF16)

        def column(j, carry):
            at = pl.multiple_of(j * LANES, LANES)
            at_v = pl.multiple_of(F + j * LANES, LANES)
            lhs = hin[s].reshape(seq, D)
            wg = gvb[:, :, :, pl.ds(at, LANES)].reshape(D, LANES)
            wv = gvb[:, :, :, pl.ds(at_v, LANES)].reshape(D, LANES)
            both = jnp.dot(lhs, jnp.concatenate([wg, wv], axis=1), preferred_element_type=F32)
            tap = taps[:, pl.ds(pl.multiple_of(q * F + j * LANES, LANES), LANES)].astype(F32)
            hid[s, :, pl.ds(at, LANES)] = finish(both[:, :LANES], both[:, LANES:], tap)
            return carry

        lax.fori_loop(0, F // LANES, column, 0)
        lhs = hin[s].reshape(seq, D)
        both = jnp.dot(lhs, gvb[:, :, :, 2 * F:].reshape(D, MW), preferred_element_type=F32)
        tail = taps[:, 2 * F:2 * F + 2 * rem].astype(F32)
        tail = jnp.where(q == 0, tail[:, :rem], tail[:, rem:])
        hid[s, :, F:] = finish(both[:, :rem], both[:, MW // 2:MW // 2 + rem], tail)

    with scope("gate_value0"):
        gate_value(0)
    with scope("relay_dn_a"):
        for a in range(DN, DN + DN_PIECES):
            relay(a, 1)
    with scope("gate_value1"):
        gate_value(1)

    groups = [(i, g) for i in range(nz) for g in range(len(subs))]
    sc = {j: [tsem() for _ in range(2)] for j in groups}
    sx = {j: [[tsem() for _ in range(nx)] for _ in range(2)] for j in groups}
    zbase = tslot[0]
    tslot[0] += nz * ny
    turns = (1 - q, q)
    split = len(subs) > 1

    def down(j):
        i, g = j
        zz = zsrc(i)
        for k, s in enumerate(turns):
            for n, e in enumerate(subs[g]):
                yy = lax.rem(y + e, ny) if split else e
                part = jnp.dot(hid[s], dnb[zz, yy], preferred_element_type=F32).astype(BF16)
                for b in range(nx * 2):
                    pb[b % 2, i, g, s, b // 2, :, n * cw:(n + 1) * cw] = part[b * R:(b + 1) * R]
            send(pb.at[1 - c, i, g, s], rb.at[i, g, s], *sc[j][k], cpeer)

    def over_x(j):
        i, g = j
        for k, s in enumerate(turns):
            arrived(rb.at[i, g, s], *sc[j][k], cpeer)
            for b in range(nx):
                ab[i, g, s, b] = (pb[c, i, g, s, b].astype(F32) + rb[i, g, s, b].astype(F32)).astype(BF16)
            for d in range(1, nx):
                send(ab.at[i, g, s, lax.rem(x + d, nx)], xr.at[i, g, d - 1, s], *sx[j][k][d], xpeer(d))

    def place(j):
        i, g = j
        return zsrc(i), (lax.rem(y + subs[g][0], ny) if split else 0)

    def over_z(j):
        i, g = j
        zz, gg = place(j)
        for k, s in enumerate(turns):
            for d in range(1, nx):
                arrived(xr.at[i, g, d - 1, s], *sx[j][k][d], xpeer(d))
            acc = ab[i, g, s, x].astype(F32)
            for d in range(1, nx):
                acc = acc + xr[i, g, d - 1, s].astype(F32)
            zb[zz, gg, s] = acc.astype(BF16)
            if k == 0:
                n = zz * ny + gg
                send(zb.at[zz, gg, s], zr.at[zz, gg], ts.at[zbase + n], trs.at[zbase + n], ppeer)

    crossed, summed_up = [], []
    early = len(pending)

    def drain(n):
        for copy, cond in pending[:n]:
            when(cond, lambda copy=copy: copy.wait_send())
        del pending[:n]


    def flush(keep_x, keep_z):
        while len(crossed) > keep_x:
            j = crossed.pop(0)
            over_x(j)
            summed_up.append(j)
        while len(summed_up) > keep_z:
            over_z(summed_up.pop(0))

    for i in range(nz):
        for g in range(len(subs)):
            if (i, g) == (nz - 1, 0):
                with scope("drain"):
                    drain(early)
            with scope(f"complete_dn{i}{g}"):
                for e in subs[g]:
                    if not split and e == 0:
                        for b in range(1, ny):
                            for a in range(DN, DN + DN_PIECES):
                                complete(a, i, b)
                    if split and e > 0:
                        for a in range(DN, DN + DN_PIECES):
                            complete(a, i, ny - e)
            with scope(f"down{i}{g}"):
                down((i, g))
            crossed.append((i, g))
            flush(1, 2)
        if 0 < i + 1 < nz and i >= 1:
            pass
        if i + 2 < nz:
            with scope(f"relay_dn{i + 2}"):
                for a in range(DN, DN + DN_PIECES):
                    relay(a, i + 2)
    with scope("tail_x"):
        flush(0, 0)
    with scope("tail_z"):
        for zz in range(nz):
            for gg in range(len(subs)):
                n = zz * ny + gg
                arrived(zr.at[zz, gg], ts.at[zbase + n], trs.at[zbase + n], ppeer)
    with scope("final"):
        ffn_out = jnp.concatenate(
            [zb[zz, gg, q].astype(F32) + zr[zz, gg].astype(F32) for zz in range(nz) for gg in range(len(subs))],
            axis=1,
        )
        out[...] = (
            normalize(RESIDUAL_SCALE * mid[...].astype(F32) + ffn_out) * ogain[...].astype(F32)
        ).astype(BF16)
    with scope("drain_end"):
        drain(len(pending))


def shards(nf, nt, ny, tokens, gate_proj, signal_proj, spatial, signal_gain, mixer_out, mixer_gain, ffn_gate, ffn_value, conv_taps, ffn_down, output_gain):
    nz = nf // ny
    nx = nt // 2
    R, D = tokens.shape
    K, C = gate_proj.shape
    H = ffn_gate.shape[1]
    full = H // (2 * LANES) * LANES
    rem = H // 2 - full
    W = full + rem
    MW = -(-2 * rem // LANES) * LANES
    cw = mixer_out.shape[1]
    seq = nx * 2 * R
    subs = [(e,) for e in range(ny)] if cw % LANES == 0 else [tuple(range(ny))]
    gw = cw * len(subs[0])
    ns = len(subs)
    packed = bool(C % LANES or (2 * rem) % LANES)
    if packed:
        gp = jnp.concatenate([gate_proj, signal_proj], axis=1)
        gt, vt = ffn_gate[:, 2 * full:], ffn_value[:, 2 * full:]
    else:
        gp, gt, vt = gate_proj, ffn_gate, ffn_value

    vm = pltpu.VMEM
    n_w = GV_PIECES + DN_PIECES
    dma = pltpu.SemaphoreType.DMA
    n_t = 2 * nx + 2 * nx + 1 + nx + 1 + 4 * nx + nz * ns * (2 + 2 * nx) + nz * ny
    scratch = [
        vm((nz, ny, K, 2 * C), BF16),
        vm((nz, ny) + mixer_out.shape, BF16),
        vm((nz, ny, K, 2 * full + MW), BF16),
        vm((nz, ny, W, cw), BF16),
        vm((2, K, 2 * rem), BF16),
        vm((2, K, MW), BF16),
        vm((nx, 2, R, D), BF16),
        vm((2 * nx, 8, seq), F32),
        vm((2, nx, R, D), BF16),
        vm((nx, R, D), BF16),
        vm((nx, R, D), BF16),
        vm((nx - 1, R, D), BF16),
        vm((R, D), BF16),
        vm((2, nx, 2, R, D), BF16),
        vm((2, seq, W), BF16),
        vm((2, nz, ns, 2, nx, R, gw), BF16),
        vm((nz, ns, 2, nx, R, gw), BF16),
        vm((nz, ns, 2, nx, R, gw), BF16),
        vm((nz, ns, nx - 1, 2, R, gw), BF16),
        vm((nz, ns, 2, R, gw), BF16),
        vm((nz, ns, R, gw), BF16),
        dma((32,)),
        dma((nz,)),
        dma((nz,)),
        dma((nz, ny)),
        dma((nz, ny)),
        dma((nz,)),
        dma((nz,)),
        dma((nz, ny)),
        dma((nz, ny)),
        dma((n_w, nz)),
        dma((n_w, nz)),
        dma((n_w, nz, ny)),
        dma((n_w, nz, ny)),
        dma((n_t,)),
        dma((n_t,)),
    ]
    here, there = pl.BlockSpec(memory_space=pltpu.VMEM), pl.BlockSpec(memory_space=pl.ANY)
    return pl.pallas_call(
        functools.partial(kernel, nz, ny, nx, full, rem, subs, packed),
        out_shape=jax.ShapeDtypeStruct((R, D), BF16),
        in_specs=[here] + [there] * 8 + [here] * 5,
        out_specs=here,
        scratch_shapes=scratch,
        compiler_params=pltpu.CompilerParams(
            collective_id=0, has_side_effects=True, vmem_limit_bytes=67043328
        ),
    )(
        tokens, gp, signal_proj, mixer_out, ffn_gate, ffn_value, gt, vt, ffn_down, spatial,
        signal_gain[None], mixer_gain[None], conv_taps, output_gain[None],
    )


def solution(mesh):
    nf, nt = mesh.shape["fs"], mesh.shape["tp"]
    ny = 2 ** (int(math.log2(nf // 2)) // 2)
    in_specs = (
        P(("fs", "tp"), None),
        P("fs", "tp"),
        P("fs", "tp"),
        P(),
        P("tp"),
        P("tp", "fs"),
        P(),
        P("fs", "tp"),
        P("fs", "tp"),
        P(None, "tp"),
        P("tp", "fs"),
        P(),
    )
    return jax.shard_map(
        functools.partial(shards, nf, nt, ny),
        mesh=mesh,
        in_specs=in_specs,
        out_specs=P(("fs", "tp"), None),
        check_vma=False,
    )
```

```python
import functools
import math

import jax
import jax.numpy as jnp
from jax import lax
from jax.experimental import pallas as pl
from jax.experimental.pallas import tpu as pltpu
from jax.sharding import PartitionSpec as P

MIX_WIDTH = 512
HEAD_SIZE = 128
BLOCK = 128
SEGMENT = 64
LANES = 128
TILES = 5
DN_PIECES = 2
KEEP_X, KEEP_Z = 1, 4
EPSILON = 1e-05
RESIDUAL_SCALE = math.sqrt(2.0)
MESH = pl.DeviceIdType.MESH
F32 = jnp.float32
BF16 = jnp.bfloat16


def normalize(values):
    row_mean = jnp.mean(values, axis=-1, keepdims=True)
    centred = values - row_mean
    spread = jnp.mean(centred * centred, axis=-1, keepdims=True)
    return centred * lax.rsqrt(spread + EPSILON)


def wide(gain):
    return gain[...].astype(F32)[None]


def plan(*words):
    return tuple(
        (w[0], int(w[1], 16), d) for w in words for d in ((1, 2, 3) if w[2] == "*" else (int(w[2]),))
    )


PLAN_Y0 = plan("o00")
PLAN_Y = plan("o10", "o20", "o30", "o40", "o50")
PLAN_FIRST = plan()
PLAN_M0 = plan("m00", "m10", "m20")
PLAN_M = plan()
PLAN_0 = plan("i01", "i02", "w00", "i11", "i12", "w10", "i21", "i22", "w20")
PLAN_A = plan("r01", "r02", "r03", "r11", "n30")
PLAN_B = plan("i31", "n40", "i41", "n50", "i51", "r12", "r21", "r13", "r22", "r23")
PLAN_C = plan("e30", "r31", "o60", "o70")
PLAN_D = plan("e40", "r41", "e50", "i61", "n60", "r51", "r32", "r33", "i71", "e60", "r42", "r43", "n70", "e70", "r52", "r53")
PLAN_E = {0: plan("r61"), 2: plan("r71")}
PLAN_H = {(0, 0): plan("r62"), (0, 1): plan("r63"), (1, 0): plan("r72"), (1, 1): plan("r73")}


def kernel(
    nz, ny, nx, full, rem, subs, packed, dn_pieces,
    tok, gp, sp_, mo, fg, fv, gt, vt, dn, spatial, sgain, mgain, taps, ogain,
    out,
    gsb, mob, gvb, gtb, dnb, tails, mixed, xin, stat, pm, prc, abm, pxr, mid, hin, hid, pb, rb, ab, xr, zb, zr,
    loc_sem, gzr, mzr, gvr, gvy, dnr, shared, ts,
):
    R, D = tok.shape
    C, cw = mo.shape
    K = fg.shape[0]
    F = full
    W = full + rem
    MW = mixed.shape[2]
    f = lax.axis_index("fs")
    t = lax.axis_index("tp")
    z, y = f // ny, f % ny
    x, c = t // 2, t % 2
    q = z % 2
    seq = nx * 2 * R
    gw = ny * cw

    def zsrc(d):
        zz = z
        for bit in (1 << k for k in range(d.bit_length())):
            if d & bit:
                zz = zz + bit - 2 * bit * ((z // bit) % 2)
        return zz

    def zpeer(d):
        return (zsrc(d) * ny + y, t)

    inner = ((z + 1) // 2) % 2

    def source(k):
        if nz != 4 or k < 2:
            return k, zsrc(k)
        return (3 - inner, 3 - 3 * (z // 2)) if k == 2 else (2 + inner, 2 - z // 2)

    def ypeer(e):
        return (z * ny + lax.rem(y + e, ny), t)

    def xpeer(d):
        return (f, lax.rem(x + d, nx) * 2 + c)

    def tpeer(d, e):
        return (f, lax.rem(x + d, nx) * 2 + (c if e == 0 else 1 - c))

    cpeer = (f, x * 2 + 1 - c)
    ppeer = ((z + 1 - 2 * q) * ny + y, t)

    def ysrc(e):
        return lax.rem(y + ny - e, ny)

    def xsrc(d):
        return lax.rem(x + nx - d, nx)

    names = {}

    def common(name):
        return shared.at[names.setdefault(name, len(names))]

    def remote(src, dst, ssem, rsem, to):
        return pltpu.make_async_remote_copy(
            src_ref=src, dst_ref=dst, send_sem=ssem, recv_sem=rsem, device_id=to, device_id_type=MESH
        )

    def send(kind, src, dst, rsem, to):
        remote(src, dst, common(kind), rsem, to).start()

    def arrived(dst, rsem):
        pltpu.make_async_copy(dst, dst, rsem).wait()

    def sent(kind, whole):
        pltpu.make_async_copy(whole, whole, common(kind)).wait()

    scope = jax.named_scope
    tslot = [0]

    def tsem():
        k = tslot[0]
        tslot[0] += 1
        return ts.at[k]

    dn_rows = W // dn_pieces
    tiles = F // LANES
    DN = tiles + 1

    def parts(a, h, zz, yy):
        if a < tiles:
            at = pl.ds(pl.multiple_of(h * F + a * LANES, LANES), LANES)
            dst = gvb.at[a, zz, yy]
            return [(fg.at[:, at], dst.at[:, pl.ds(0, LANES)]), (fv.at[:, at], dst.at[:, pl.ds(LANES, LANES)])]
        if a < DN:
            return [(mixed.at[h], gtb.at[zz, yy])]
        lo, hi = (a - DN) * dn_rows, (a - DN + 1) * dn_rows
        dst = dnb.at[zz, yy]
        found = []
        if lo < F:
            n = min(hi, F) - lo
            found.append((dn.at[pl.ds(pl.multiple_of(h * F + lo, 16), n)], dst.at[pl.ds(lo, n)]))
        if hi > F:
            s = max(lo, F)
            n = hi - s
            found.append(
                (dn.at[pl.ds(pl.multiple_of(2 * F + h * rem + s - F, 16), n)], dst.at[pl.ds(s, n)])
            )
        return found

    def slot(a, zz, yy):
        if a < tiles:
            return gvb.at[a, zz, yy]
        if a < DN:
            return gtb.at[zz, yy]
        return dnb.at[zz, yy, pl.ds((a - DN) * dn_rows, dn_rows)]

    def fetch(k, src, dst):
        pltpu.make_async_copy(src, dst, loc_sem.at[k]).start()

    def ready(k, whole):
        pltpu.make_async_copy(whole, whole, loc_sem.at[k]).wait()

    GS, MO, TAILS, GV, DOWN = range(5)
    if packed:
        fetch(GS, gp, gsb.at[z, y])
    else:
        fetch(GS, gp, gsb.at[z, y, :, pl.ds(0, C)])
        fetch(GS, sp_, gsb.at[z, y, :, pl.ds(C, C)])
    fetch(MO, mo, mob.at[z, y])
    T = tails.shape[2]
    if packed:
        fetch(TAILS, gt, tails.at[0])
        fetch(TAILS, vt, tails.at[1])
    else:
        fetch(TAILS, gt.at[:, pl.ds(2 * F, T)], tails.at[0])
        fetch(TAILS, vt.at[:, pl.ds(2 * F, T)], tails.at[1])
    for a in range(tiles):
        for src, dst in parts(a, q, z, y):
            fetch(GV, src, dst)
    for a in range(DN, DN + dn_pieces):
        for src, dst in parts(a, q, z, y):
            fetch(DOWN, src, dst)

    barrier = pltpu.get_barrier_semaphore()
    peers = [zpeer(d) for d in range(1, nz)] + [ypeer(e) for e in range(1, ny)]
    peers += [tpeer(d, e) for d in range(nx) for e in range(2) if d + e]
    for p in peers:
        pl.semaphore_signal(barrier, inc=1, device_id=p, device_id_type=MESH)

    ready(TAILS, tails)
    for h in range(2):
        for k in range(2):
            mixed[h, :, k * (MW // 2):k * (MW // 2) + rem] = tails[k, :, h * rem:(h + 1) * rem]
    for k in range(2):
        part = tails[k].astype(F32)
        part = jnp.where(q == 0, part[:, :rem], part[:, rem:2 * rem]).astype(BF16)
        gtb[z, y, :, k * (MW // 2):k * (MW // 2) + rem] = part
    ready(GS, gsb.at[z, y])
    ready(MO, mob.at[z, y])
    pl.semaphore_wait(barrier, len(peers))

    def issue_z(a, d):
        for src, dst in parts(a, zsrc(d) % 2, z, y):
            remote(src, dst, common(family(a) + "_z"), z_sem(a, d), zpeer(d)).start()

    def z_sem(a, d):
        return gvr.at[a, d] if a < DN else dnr.at[a - DN, d]

    def y_sem(a, d, e):
        return gvy.at[a, e] if a < DN else dnr.at[dn_pieces + e - 1, d]

    def family(a):
        return "gv" if a < tiles else "gt" if a < DN else "dn"

    def issue_y(a):
        for e in range(1, ny):
            send(family(a) + "_y", slot(a, z, y), slot(a, z, y), y_sem(a, 0, e), ypeer(e))

    def relay(a, k):
        d, zz = source(k)
        arrived(slot(a, zz, y), z_sem(a, d))
        for e in range(1, ny):
            send(family(a) + "_y", slot(a, zz, y), slot(a, zz, y), y_sem(a, d, e), ypeer(e))

    bits = [1 << k for k in reversed(range((nz - 1).bit_length()))]

    def spread(kind, buf, d, rsem):
        src = zsrc(d)
        for bit in bits:
            if d == 0 or bit < (d & -d):
                send(kind, buf(src), buf(src), rsem.at[d | bit], zpeer(bit))

    def issue_far(a, what):
        if nz != 4:
            for d in range(2, nz):
                if (what == "n") == (d == 2) and what != "w" and (what != "m" or d > 2):
                    issue_z(a, d)
            return
        if what in "mw":
            pl.when(inner == (1 if what == "m" else 0))(lambda: issue_z(a, 3))
            return
        row = 2 - z // 2 if what == "n" else 3 - 3 * (z // 2)
        d = 2 + inner if what == "n" else 3 - inner
        for src, dst in parts(a, row % 2, z, y):
            remote(src, dst, common(family(a) + "_z"), z_sem(a, d), (row * ny + y, t)).start()

    def steps(plan):
        for what, piece, d in plan:
            if piece < TILES and piece >= tiles:
                continue
            a = piece if piece < TILES else piece - TILES + tiles
            if what == "o":
                issue_y(a)
            elif what in "nemw":
                issue_far(a, what)
            for dd in range(1, nz):
                if dd == d or (d == 3 and dd > 3):
                    (relay if what == "r" else issue_z)(a, dd)

    def gs_block(src):
        return gsb.at[src, y]

    def mo_block(src):
        return mob.at[src]

    spread("gs_z", gs_block, 0, gzr)
    for e in range(1, ny):
        send("mo_y", mob.at[z, y], mob.at[z, y], common(f"mo_y{e}r"), ypeer(e))
    for e in range(1, ny):
        send("gs_y", gsb.at[z, y], gsb.at[z, y], common(f"gs_y{e}r"), ypeer(e))
    ready(GV, gvb.at[:, z, y])
    steps(PLAN_Y0)
    steps(PLAN_FIRST)

    xin[x, c] = normalize(tok[...].astype(F32)).astype(BF16)
    s1 = [tsem() for _ in range(nx)]
    for d in range(1, nx):
        send("xin_x", xin.at[x, c], xin.at[x, c], s1[d], xpeer(d))
    send("xin_c", xin.at[x, c], xin.at[x, c], common("xin_cr"), cpeer)

    with scope("mo_y"):
        for e in range(1, ny):
            arrived(mob.at[z, ysrc(e)], common(f"mo_y{e}r"))
    spread("mo_z", mo_block, 0, mzr)
    steps(PLAN_M0)
    for d in range(1, nz):
        with scope(f"relay_gs{d}"):
            arrived(gs_block(zsrc(d)), gzr.at[d])
            spread("gs_z", gs_block, d, gzr)
            for e in range(1, ny):
                send("gs_y", gs_block(zsrc(d)), gs_block(zsrc(d)), common(f"gs_y{e}r"), ypeer(e))
    steps(PLAN_M)
    for d in range(1, nz):
        with scope(f"relay_mo{d}"):
            arrived(mo_block(zsrc(d)), mzr.at[d])
            spread("mo_z", mo_block, d, mzr)
    with scope("first_z"):
        steps(PLAN_0)
    ready(DOWN, dnb.at[z, y])
    steps(PLAN_Y)
    with scope("xin"):
        for d in range(1, nx):
            arrived(xin.at[xsrc(d), c], s1[d])
            send("xin_c", xin.at[xsrc(d), c], xin.at[xsrc(d), c], common("xin_cr"), cpeer)
        arrived(xin.at[:, 1 - c], common("xin_cr"))
    with scope("complete_gs"):
        for e in range(1, ny):
            arrived(gsb.at[:, ysrc(e)], common(f"gs_y{e}r"))

    with scope("mix_in"):
        pre = jnp.dot(xin[...].reshape(seq, D), gsb[...].reshape(D, 2 * C), preferred_element_type=F32)
        branch_signal = jax.nn.gelu(pre[:, C:])
        total = jnp.sum(branch_signal, axis=1, keepdims=True)
        square = jnp.sum(branch_signal * branch_signal, axis=1, keepdims=True)
        lane = lax.broadcasted_iota(jnp.int32, (seq, LANES), 1)
        stat[0] = jnp.where(lane == 0, total, square).T[:8]
    others = [(d, e) for d in range(nx) for e in range(2) if d + e]
    sx = {}
    for d, e in others:
        sx[d, e] = tsem()
        send("stat", stat.at[0], stat.at[2 * d + e], sx[d, e], tpeer(d, e))
    branch_gate = jax.nn.gelu(pre[:, :C])
    with scope("stats"):
        summed = stat[0]
        for d, e in others:
            arrived(stat.at[2 * d + e], sx[d, e])
            summed = summed + stat[2 * d + e]
    with scope("mix_out"):
        back = summed.T
        row_mean = back[:, 0:1] / MIX_WIDTH
        spread = back[:, 1:2] / MIX_WIDTH - row_mean * row_mean
        spatial_input = (
            (branch_signal - row_mean) * lax.rsqrt(spread + EPSILON) * wide(sgain)
        ).astype(BF16)
        rows_i = lax.broadcasted_iota(jnp.int32, (BLOCK, BLOCK), 0) // SEGMENT
        cols_i = lax.broadcasted_iota(jnp.int32, (BLOCK, BLOCK), 1) // SEGMENT
        own = spatial[t * C // HEAD_SIZE]
        own = jnp.where(cols_i <= rows_i, own, jnp.zeros_like(own))
        gated = jnp.concatenate(
            [
                branch_gate[b * BLOCK:(b + 1) * BLOCK]
                * jnp.dot(own, spatial_input[b * BLOCK:(b + 1) * BLOCK], preferred_element_type=F32)
                for b in range(seq // BLOCK)
            ],
            axis=0,
        ).astype(BF16)
        for k in range(nz * ny):
            part = jnp.dot(gated, mob[k // ny, k % ny], preferred_element_type=F32).astype(BF16)
            for b in range(nx * 2):
                pm[b % 2, b // 2, :, k * cw:(k + 1) * cw] = part[b * R:(b + 1) * R]
    sc = tsem()
    send("pm", pm.at[1 - c], prc, sc, cpeer)
    with scope("mix_core"):
        arrived(prc, sc)
    for b in range(nx):
        abm[b] = (pm[c, b].astype(F32) + prc[b].astype(F32)).astype(BF16)
    sx = [tsem() for _ in range(nx)]
    for d in range(1, nx):
        send("abm", abm.at[lax.rem(x + d, nx)], pxr.at[d - 1], sx[d], xpeer(d))
    with scope("relay_gv0"):
        steps(PLAN_A)
    with scope("mix_x"):
        for d in range(1, nx):
            arrived(pxr.at[d - 1], sx[d])
    with scope("mid"):
        mix_out = pm[c, x].astype(F32) + prc[x].astype(F32)
        for d in range(1, nx):
            mix_out = mix_out + pxr[d - 1].astype(F32)
        mid[...] = (
            normalize(RESIDUAL_SCALE * tok[...].astype(F32) + mix_out) * wide(mgain)
        ).astype(BF16)
        hin[q, x, c] = normalize(mid[...].astype(F32)).astype(BF16)

    sp = tsem()
    send("hin_z", hin.at[q, x, c], hin.at[q, x, c], sp, ppeer)
    sx = [[tsem() for _ in range(nx)] for _ in range(2)]

    def rows_out(k, s):
        for d in range(1, nx):
            send("hin_x", hin.at[s, x, c], hin.at[s, x, c], sx[k][d], xpeer(d))
        send("hin_c", hin.at[s, x, c], hin.at[s, x, c], common("hin_cr"), cpeer)

    def rows_over(k, s):
        for d in range(1, nx):
            arrived(hin.at[s, xsrc(d), c], sx[k][d])
            send("hin_c", hin.at[s, xsrc(d), c], hin.at[s, xsrc(d), c], common("hin_cr"), cpeer)

    rows_out(0, q)
    with scope("relay_b"):
        steps(PLAN_B)
    with scope("rows_x0"):
        rows_over(0, q)
    with scope("relay_c"):
        steps(PLAN_C)
    with scope("pair_rows"):
        arrived(hin.at[1 - q, x, c], sp)
    rows_out(1, 1 - q)
    with scope("relay_d"):
        steps(PLAN_D)
    with scope("rows_x1"):
        rows_over(1, 1 - q)
    with scope("rows_core"):
        arrived(hin.at[:, :, 1 - c], common("hin_cr"))
    def gate_value(a):
        lhs_rows = (hin[s].reshape(seq, D) for s in range(2))
        if a < tiles:
            weights = gvb[a].reshape(D, 2 * LANES)
            tap = taps[:, pl.ds(pl.multiple_of(q * F + a * LANES, LANES), LANES)].astype(F32)
            n, at = LANES, LANES
        else:
            weights = gtb[...].reshape(D, MW)
            tap = taps[:, 2 * F:2 * F + 2 * rem].astype(F32)
            tap = jnp.where(q == 0, tap[:, :rem], tap[:, rem:])
            n, at = rem, MW // 2
        for s, lhs in enumerate(lhs_rows):
            both = jnp.dot(lhs, weights, preferred_element_type=F32)
            gate, value = both[:, :n], both[:, at:at + n]
            row = lax.broadcasted_iota(jnp.int32, gate.shape, 0)
            one = jnp.where(row >= 1, pltpu.roll(gate, 1, 0), 0.0)
            two = jnp.where(row >= 2, pltpu.roll(gate, 2, 0), 0.0)
            conv = tap[0:1] * two + tap[1:2] * one + tap[2:3] * gate
            hid[s, :, a * LANES:a * LANES + n] = (jax.nn.silu(conv) * value).astype(BF16)

    for a in range(DN):
        with scope(f"complete_gv{a}"):
            for e in range(1, ny):
                whole = gvb.at[a, :, ysrc(e)] if a < tiles else gtb.at[:, ysrc(e)]
                arrived(whole, gvy.at[a, e])
        with scope(f"gate_value{a}"):
            gate_value(a)
        with scope("relay_e"):
            steps(PLAN_E.get(a if a < tiles else TILES, ()))

    groups = sorted(
        ((i, g) for i in range(nz) for g in range(len(subs))),
        key=lambda j: (j[0] >= nz // 2, j[1] > 0 and j[0] >= nz // 2, j),
    )
    sc = {j: [tsem() for _ in range(2)] for j in groups}
    sx = {j: [[tsem() for _ in range(nx)] for _ in range(2)] for j in groups}
    turns = (1 - q, q)
    split = len(subs) > 1

    def down(item):
        (i, g), k = item
        s, zz = turns[k], source(i)[1]
        for n, e in enumerate(subs[g]):
            yy = lax.rem(y + e, ny) if split else e
            part = jnp.dot(hid[s], dnb[zz, yy], preferred_element_type=F32).astype(BF16)
            for b in range(nx * 2):
                pb[b % 2, i, g, s, b // 2, :, n * cw:(n + 1) * cw] = part[b * R:(b + 1) * R]
        send("pb", pb.at[1 - c, i, g, s], rb.at[i, g, s], sc[i, g][k], cpeer)
        crossed.append(item)

    def over_x(item):
        (i, g), k = item
        s = turns[k]
        arrived(rb.at[i, g, s], sc[i, g][k])
        for b in range(nx):
            ab[i, g, s, b] = (pb[c, i, g, s, b].astype(F32) + rb[i, g, s, b].astype(F32)).astype(BF16)
        for d in range(1, nx):
            send("ab", ab.at[i, g, s, lax.rem(x + d, nx)], xr.at[i, g, d - 1, s], sx[i, g][k][d], xpeer(d))

    def over_z(item):
        (i, g), k = item
        s, zz = turns[k], source(i)[1]
        gg = lax.rem(y + subs[g][0], ny) if split else 0
        for d in range(1, nx):
            arrived(xr.at[i, g, d - 1, s], sx[i, g][k][d])
        acc = ab[i, g, s, x].astype(F32)
        for d in range(1, nx):
            acc = acc + xr[i, g, d - 1, s].astype(F32)
        zb[zz, gg, s] = acc.astype(BF16)
        if k == 0:
            send("zb", zb.at[zz, gg, s], zr.at[zz, gg], common("zbr"), ppeer)

    crossed, summed_up = [], []
    def flush(keep_x, keep_z):
        while len(crossed) > keep_x:
            j = crossed.pop(0)
            over_x(j)
            summed_up.append(j)
        while len(summed_up) > keep_z:
            over_z(summed_up.pop(0))

    def complete_dn(j):
        i, g = j
        with scope(f"complete_dn{i}{g}"):
            for e in range(1, ny):
                if (split and e in subs[g]) or not split:
                    b = ny - e if split else e
                    d, zz = source(i)
                    arrived(dnb.at[zz, ysrc(b)], dnr.at[dn_pieces + b - 1, d])

    for j in groups:
        complete_dn(j)
        with scope(f"down{j[0]}{j[1]}"):
            down((j, 0))
            down((j, 1))
        with scope(f"relay_h{j[0]}"):
            steps(PLAN_H.get(j, ()) if split else PLAN_H.get((j[0], 0), ()) + PLAN_H.get((j[0], 1), ()))
        with scope(f"flush{j[0]}{j[1]}"):
            flush(KEEP_X, KEEP_Z)
    with scope("tail_x"):
        flush(0, 0)
    with scope("tail_z"):
        arrived(zr, common("zbr"))
    with scope("final"):
        ffn_out = jnp.concatenate(
            [zb[zz, gg, q].astype(F32) + zr[zz, gg].astype(F32) for zz in range(nz) for gg in range(len(subs))],
            axis=1,
        )
        out[...] = (
            normalize(RESIDUAL_SCALE * mid[...].astype(F32) + ffn_out) * wide(ogain)
        ).astype(BF16)
    with scope("drain_end"):
        sent("gs_z", gsb.at[pl.ds(0, nz - 1), y])
        sent("mo_z", mob.at[pl.ds(0, nz - 1)])
        far = pl.ds(0, nz - 1)
        sent("gv_z", gvb.at[:, far, y])
        sent("gt_z", gtb.at[far, y])
        sent("dn_z", dnb.at[far, y])
        over_y = pl.ds(0, ny - 1)
        sent("mo_y", mob.at[z, over_y])
        sent("gs_y", gsb.at[:, over_y])
        sent("gv_y", gvb.at[:, :, over_y])
        sent("gt_y", gtb.at[:, over_y])
        sent("dn_y", dnb.at[:, over_y])
        sent("xin_x", xin.at[pl.ds(0, nx - 1), 0])
        sent("xin_c", xin.at[:, c])
        sent("stat", stat.at[pl.ds(0, 2 * nx - 1)])
        sent("pm", prc)
        sent("abm", pxr)
        sent("hin_z", hin.at[q, x, c])
        sent("hin_x", hin.at[:, pl.ds(0, nx - 1), c])
        sent("hin_c", hin.at[:, :, c])
        sent("pb", rb)
        sent("ab", xr)
        sent("zb", zr)


def shards(nf, nt, ny, tokens, gate_proj, signal_proj, spatial, signal_gain, mixer_out, mixer_gain, ffn_gate, ffn_value, conv_taps, ffn_down, output_gain):
    nz = nf // ny
    nx = nt // 2
    R, D = tokens.shape
    K, C = gate_proj.shape
    H = ffn_gate.shape[1]
    full = H // (2 * LANES) * LANES
    rem = H // 2 - full
    W = full + rem
    MW = -(-2 * rem // LANES) * LANES
    cw = mixer_out.shape[1]
    seq = nx * 2 * R
    subs = [(e,) for e in range(ny)] if cw % LANES == 0 else [tuple(range(ny))]
    gw = cw * len(subs[0])
    ns = len(subs)
    dn_pieces = DN_PIECES
    packed = bool(C % LANES or (2 * rem) % LANES)
    if packed:
        gp = jnp.concatenate([gate_proj, signal_proj], axis=1)
        gt, vt = ffn_gate[:, 2 * full:], ffn_value[:, 2 * full:]
    else:
        gp, gt, vt = gate_proj, ffn_gate, ffn_value

    vm = pltpu.VMEM
    dma = pltpu.SemaphoreType.DMA
    n_t = 6 * nx + 2 + nz * ns * (2 + 2 * nx)
    scratch = [
        vm((nz, ny, K, 2 * C), BF16),
        vm((nz, ny) + mixer_out.shape, BF16),
        vm((full // LANES, nz, ny, K, 2 * LANES), BF16),
        vm((nz, ny, K, MW), BF16),
        vm((nz, ny, W, cw), BF16),
        vm((2, K, 2 * rem), BF16),
        vm((2, K, MW), BF16),
        vm((nx, 2, R, D), BF16),
        vm((2 * nx, 8, seq), F32),
        vm((2, nx, R, D), BF16),
        vm((nx, R, D), BF16),
        vm((nx, R, D), BF16),
        vm((nx - 1, R, D), BF16),
        vm((R, D), BF16),
        vm((2, nx, 2, R, D), BF16),
        vm((2, seq, W), BF16),
        vm((2, nz, ns, 2, nx, R, gw), BF16),
        vm((nz, ns, 2, nx, R, gw), BF16),
        vm((nz, ns, 2, nx, R, gw), BF16),
        vm((nz, ns, nx - 1, 2, R, gw), BF16),
        vm((nz, ns, 2, R, gw), BF16),
        vm((nz, ns, R, gw), BF16),
        dma((5,)),
        dma((nz,)),
        dma((nz,)),
        dma((full // LANES + 1, nz)),
        dma((full // LANES + 1, ny)),
        dma((dn_pieces + ny - 1, nz)),
        dma((24 + 2 * (ny - 1),)),
        dma((n_t,)),
    ]
    here, there = pl.BlockSpec(memory_space=pltpu.VMEM), pl.BlockSpec(memory_space=pl.ANY)
    return pl.pallas_call(
        functools.partial(kernel, nz, ny, nx, full, rem, subs, packed, dn_pieces),
        out_shape=jax.ShapeDtypeStruct((R, D), BF16),
        in_specs=[here] + [there] * 8 + [here] * 5,
        out_specs=here,
        scratch_shapes=scratch,
        compiler_params=pltpu.CompilerParams(
            collective_id=0, has_side_effects=True, vmem_limit_bytes=67043328
        ),
    )(
        tokens, gp, signal_proj, mixer_out, ffn_gate, ffn_value, gt, vt, ffn_down, spatial,
        signal_gain, mixer_gain, conv_taps, output_gain,
    )


def solution(mesh):
    nf, nt = mesh.shape["fs"], mesh.shape["tp"]
    ny = 2 ** (int(math.log2(nf // 2)) // 2)
    in_specs = (
        P(("fs", "tp"), None),
        P("fs", "tp"),
        P("fs", "tp"),
        P(),
        P("tp"),
        P("tp", "fs"),
        P(),
        P("fs", "tp"),
        P("fs", "tp"),
        P(None, "tp"),
        P("tp", "fs"),
        P(),
    )
    return jax.shard_map(
        functools.partial(shards, nf, nt, ny),
        mesh=mesh,
        in_specs=in_specs,
        out_specs=P(("fs", "tp"), None),
        check_vma=False,
    )
```

```python
import functools
import math

import jax
import jax.numpy as jnp
from jax import lax
from jax.experimental import pallas as pl
from jax.experimental.pallas import tpu as pltpu
from jax.sharding import PartitionSpec as P

MIX_WIDTH = 512
HEAD_SIZE = 128
BLOCK = 128
SEGMENT = 64
LANES = 128
TILES = 5
DN_PIECES = 2
KEEP_X, KEEP_Z = 0, 4
EPSILON = 1e-05
RESIDUAL_SCALE = math.sqrt(2.0)
MESH = pl.DeviceIdType.MESH
F32 = jnp.float32
BF16 = jnp.bfloat16


def normalize(values):
    row_mean = jnp.mean(values, axis=-1, keepdims=True)
    centred = values - row_mean
    spread = jnp.mean(centred * centred, axis=-1, keepdims=True)
    return centred * lax.rsqrt(spread + EPSILON)


def wide(gain):
    return gain[...].astype(F32)[None]


def plan(*words):
    return tuple(
        (w[0], int(w[1], 16), d) for w in words for d in ((1, 2, 3) if w[2] == "*" else (int(w[2]),))
    )


PLAN_Y0 = plan("o00")
PLAN_Y = plan("o10", "o20", "o30", "o40", "o50", "o60", "o70")
PLAN_FIRST = plan()
PLAN_M0 = plan("m00", "m10", "m20")
PLAN_M = plan()
PLAN_0 = plan("i01", "i02", "w00", "i11", "i12", "w10", "i21", "i22", "w20")
PLAN_A = plan("r01", "r02", "r03", "r11", "n30")
PLAN_B = plan("i31", "n40", "i41", "n50", "i51", "r12", "r21", "r13", "r22", "r23")
PLAN_C = plan("e30", "r31")
PLAN_D = plan("e40", "r41", "e50", "n60", "r51", "i61", "r32", "e60", "r33", "i71", "n70", "r42", "r43", "e70", "r52", "r53")
PLAN_E = {1: plan("r61"), 4: plan("r71")}
PLAN_H = {(0, 0): plan("r62"), (0, 1): plan("r63"), (1, 0): plan(), (1, 1): plan("r72", "r73")}


def kernel(
    nz, ny, nx, full, rem, subs, packed, dn_pieces,
    tok, gp, sp_, mo, fg, fv, gt, vt, dn, spatial, sgain, mgain, taps, ogain,
    out,
    gsb, mob, gvb, gtb, dnb, tails, mixed, xin, stat, pm, prc, abm, pxr, mid, hin, hid, pb, rb, ab, xr, zb, zr,
    loc_sem, gzr, mzr, gvr, gvy, dnr, shared, ts,
):
    R, D = tok.shape
    C, cw = mo.shape
    K = fg.shape[0]
    F = full
    W = full + rem
    MW = mixed.shape[2]
    f = lax.axis_index("fs")
    t = lax.axis_index("tp")
    z, y = f // ny, f % ny
    x, c = t // 2, t % 2
    q = z % 2
    seq = nx * 2 * R
    gw = ny * cw

    def zsrc(d):
        zz = z
        for bit in (1 << k for k in range(d.bit_length())):
            if d & bit:
                zz = zz + bit - 2 * bit * ((z // bit) % 2)
        return zz

    def zpeer(d):
        return (zsrc(d) * ny + y, t)

    inner = ((z + 1) // 2) % 2

    def source(k):
        if nz != 4 or k < 2:
            return k, zsrc(k)
        return (3 - inner, 3 - 3 * (z // 2)) if k == 2 else (2 + inner, 2 - z // 2)

    def ypeer(e):
        return (z * ny + lax.rem(y + e, ny), t)

    def xpeer(d):
        return (f, lax.rem(x + d, nx) * 2 + c)

    def tpeer(d, e):
        return (f, lax.rem(x + d, nx) * 2 + (c if e == 0 else 1 - c))

    cpeer = (f, x * 2 + 1 - c)
    ppeer = ((z + 1 - 2 * q) * ny + y, t)

    def ysrc(e):
        return lax.rem(y + ny - e, ny)

    def xsrc(d):
        return lax.rem(x + nx - d, nx)

    names = {}

    def common(name):
        return shared.at[names.setdefault(name, len(names))]

    def remote(src, dst, ssem, rsem, to):
        return pltpu.make_async_remote_copy(
            src_ref=src, dst_ref=dst, send_sem=ssem, recv_sem=rsem, device_id=to, device_id_type=MESH
        )

    def send(kind, src, dst, rsem, to):
        remote(src, dst, common(kind), rsem, to).start()

    def arrived(dst, rsem):
        pltpu.make_async_copy(dst, dst, rsem).wait()

    def sent(kind, whole):
        pltpu.make_async_copy(whole, whole, common(kind)).wait()

    scope = jax.named_scope
    tslot = [0]

    def tsem():
        k = tslot[0]
        tslot[0] += 1
        return ts.at[k]

    dn_rows = W // dn_pieces
    tiles = F // LANES
    DN = tiles + 1

    def parts(a, h, zz, yy):
        if a < tiles:
            at = pl.ds(pl.multiple_of(h * F + a * LANES, LANES), LANES)
            dst = gvb.at[a, zz, yy]
            return [(fg.at[:, at], dst.at[:, pl.ds(0, LANES)]), (fv.at[:, at], dst.at[:, pl.ds(LANES, LANES)])]
        if a < DN:
            return [(mixed.at[h], gtb.at[zz, yy])]
        lo, hi = (a - DN) * dn_rows, (a - DN + 1) * dn_rows
        dst = dnb.at[zz, yy]
        found = []
        if lo < F:
            n = min(hi, F) - lo
            found.append((dn.at[pl.ds(pl.multiple_of(h * F + lo, 16), n)], dst.at[pl.ds(lo, n)]))
        if hi > F:
            s = max(lo, F)
            n = hi - s
            found.append(
                (dn.at[pl.ds(pl.multiple_of(2 * F + h * rem + s - F, 16), n)], dst.at[pl.ds(s, n)])
            )
        return found

    def slot(a, zz, yy):
        if a < tiles:
            return gvb.at[a, zz, yy]
        if a < DN:
            return gtb.at[zz, yy]
        return dnb.at[zz, yy, pl.ds((a - DN) * dn_rows, dn_rows)]

    def fetch(k, src, dst):
        pltpu.make_async_copy(src, dst, loc_sem.at[k]).start()

    def ready(k, whole):
        pltpu.make_async_copy(whole, whole, loc_sem.at[k]).wait()

    GS, MO, TAILS, GV, DOWN = range(5)
    if packed:
        fetch(GS, gp, gsb.at[z, y])
    else:
        fetch(GS, gp, gsb.at[z, y, :, pl.ds(0, C)])
        fetch(GS, sp_, gsb.at[z, y, :, pl.ds(C, C)])
    fetch(MO, mo, mob.at[z, y])
    T = tails.shape[2]
    if packed:
        fetch(TAILS, gt, tails.at[0])
        fetch(TAILS, vt, tails.at[1])
    else:
        fetch(TAILS, gt.at[:, pl.ds(2 * F, T)], tails.at[0])
        fetch(TAILS, vt.at[:, pl.ds(2 * F, T)], tails.at[1])
    for a in range(tiles):
        for src, dst in parts(a, q, z, y):
            fetch(GV, src, dst)
    for a in range(DN, DN + dn_pieces):
        for src, dst in parts(a, q, z, y):
            fetch(DOWN, src, dst)

    barrier = pltpu.get_barrier_semaphore()
    peers = [zpeer(d) for d in range(1, nz)] + [ypeer(e) for e in range(1, ny)]
    peers += [tpeer(d, e) for d in range(nx) for e in range(2) if d + e]
    for p in peers:
        pl.semaphore_signal(barrier, inc=1, device_id=p, device_id_type=MESH)

    ready(TAILS, tails)
    for h in range(2):
        for k in range(2):
            mixed[h, :, k * (MW // 2):k * (MW // 2) + rem] = tails[k, :, h * rem:(h + 1) * rem]
    for k in range(2):
        part = tails[k].astype(F32)
        part = jnp.where(q == 0, part[:, :rem], part[:, rem:2 * rem]).astype(BF16)
        gtb[z, y, :, k * (MW // 2):k * (MW // 2) + rem] = part
    ready(GS, gsb.at[z, y])
    ready(MO, mob.at[z, y])
    pl.semaphore_wait(barrier, len(peers))

    def issue_z(a, d):
        for src, dst in parts(a, zsrc(d) % 2, z, y):
            remote(src, dst, common(family(a) + "_z"), z_sem(a, d), zpeer(d)).start()

    def z_sem(a, d):
        return gvr.at[a, d] if a < DN else dnr.at[a - DN, d]

    def y_sem(a, d, e):
        return gvy.at[a, e] if a < DN else dnr.at[dn_pieces + e - 1, d]

    def family(a):
        return "gv" if a < tiles else "gt" if a < DN else "dn"

    def issue_y(a):
        for e in range(1, ny):
            send(family(a) + "_y", slot(a, z, y), slot(a, z, y), y_sem(a, 0, e), ypeer(e))

    def relay(a, k):
        d, zz = source(k)
        arrived(slot(a, zz, y), z_sem(a, d))
        for e in range(1, ny):
            send(family(a) + "_y", slot(a, zz, y), slot(a, zz, y), y_sem(a, d, e), ypeer(e))

    bits = [1 << k for k in reversed(range((nz - 1).bit_length()))]

    def spread(kind, buf, d, rsem):
        src = zsrc(d)
        for bit in bits:
            if d == 0 or bit < (d & -d):
                send(kind, buf(src), buf(src), rsem.at[d | bit], zpeer(bit))

    def issue_far(a, what):
        if nz != 4:
            for d in range(2, nz):
                if (what == "n") == (d == 2) and what != "w" and (what != "m" or d > 2):
                    issue_z(a, d)
            return
        if what in "mw":
            pl.when(inner == (1 if what == "m" else 0))(lambda: issue_z(a, 3))
            return
        row = 2 - z // 2 if what == "n" else 3 - 3 * (z // 2)
        d = 2 + inner if what == "n" else 3 - inner
        for src, dst in parts(a, row % 2, z, y):
            remote(src, dst, common(family(a) + "_z"), z_sem(a, d), (row * ny + y, t)).start()

    def steps(plan):
        for what, piece, d in plan:
            if piece < TILES and piece >= tiles:
                continue
            a = piece if piece < TILES else piece - TILES + tiles
            if what == "o":
                issue_y(a)
            elif what in "nemw":
                issue_far(a, what)
            for dd in range(1, nz):
                if dd == d or (d == 3 and dd > 3):
                    (relay if what == "r" else issue_z)(a, dd)

    def gs_block(src):
        return gsb.at[src, y]

    def mo_block(src):
        return mob.at[src]

    spread("gs_z", gs_block, 0, gzr)
    for e in range(1, ny):
        send("mo_y", mob.at[z, y], mob.at[z, y], common(f"mo_y{e}r"), ypeer(e))
    for e in range(1, ny):
        send("gs_y", gsb.at[z, y], gsb.at[z, y], common(f"gs_y{e}r"), ypeer(e))
    ready(GV, gvb.at[:, z, y])
    steps(PLAN_Y0)
    steps(PLAN_FIRST)

    xin[x, c] = normalize(tok[...].astype(F32)).astype(BF16)
    s1 = [tsem() for _ in range(nx)]
    for d in range(1, nx):
        send("xin_x", xin.at[x, c], xin.at[x, c], s1[d], xpeer(d))
    send("xin_c", xin.at[x, c], xin.at[x, c], common("xin_cr"), cpeer)

    with scope("mo_y"):
        for e in range(1, ny):
            arrived(mob.at[z, ysrc(e)], common(f"mo_y{e}r"))
    spread("mo_z", mo_block, 0, mzr)
    steps(PLAN_M0)
    for d in range(1, nz):
        with scope(f"relay_gs{d}"):
            arrived(gs_block(zsrc(d)), gzr.at[d])
            spread("gs_z", gs_block, d, gzr)
            for e in range(1, ny):
                send("gs_y", gs_block(zsrc(d)), gs_block(zsrc(d)), common(f"gs_y{e}r"), ypeer(e))
    steps(PLAN_M)
    for d in range(1, nz):
        with scope(f"relay_mo{d}"):
            arrived(mo_block(zsrc(d)), mzr.at[d])
            spread("mo_z", mo_block, d, mzr)
    with scope("first_z"):
        steps(PLAN_0)
    ready(DOWN, dnb.at[z, y])
    steps(PLAN_Y)
    with scope("xin"):
        for d in range(1, nx):
            arrived(xin.at[xsrc(d), c], s1[d])
            send("xin_c", xin.at[xsrc(d), c], xin.at[xsrc(d), c], common("xin_cr"), cpeer)
        arrived(xin.at[:, 1 - c], common("xin_cr"))
    with scope("complete_gs"):
        for e in range(1, ny):
            arrived(gsb.at[:, ysrc(e)], common(f"gs_y{e}r"))

    with scope("mix_in"):
        pre = jnp.dot(xin[...].reshape(seq, D), gsb[...].reshape(D, 2 * C), preferred_element_type=F32)
        branch_signal = jax.nn.gelu(pre[:, C:])
        total = jnp.sum(branch_signal, axis=1, keepdims=True)
        square = jnp.sum(branch_signal * branch_signal, axis=1, keepdims=True)
        lane = lax.broadcasted_iota(jnp.int32, (seq, LANES), 1)
        stat[0] = jnp.where(lane == 0, total, square).T[:8]
    others = [(d, e) for d in range(nx) for e in range(2) if d + e]
    sx = {}
    for d, e in others:
        sx[d, e] = tsem()
        send("stat", stat.at[0], stat.at[2 * d + e], sx[d, e], tpeer(d, e))
    branch_gate = jax.nn.gelu(pre[:, :C])
    with scope("stats"):
        summed = stat[0]
        for d, e in others:
            arrived(stat.at[2 * d + e], sx[d, e])
            summed = summed + stat[2 * d + e]
    with scope("mix_out"):
        back = summed.T
        row_mean = back[:, 0:1] / MIX_WIDTH
        spread = back[:, 1:2] / MIX_WIDTH - row_mean * row_mean
        spatial_input = (
            (branch_signal - row_mean) * lax.rsqrt(spread + EPSILON) * wide(sgain)
        ).astype(BF16)
        rows_i = lax.broadcasted_iota(jnp.int32, (BLOCK, BLOCK), 0) // SEGMENT
        cols_i = lax.broadcasted_iota(jnp.int32, (BLOCK, BLOCK), 1) // SEGMENT
        own = spatial[t * C // HEAD_SIZE]
        own = jnp.where(cols_i <= rows_i, own, jnp.zeros_like(own))
        gated = jnp.concatenate(
            [
                branch_gate[b * BLOCK:(b + 1) * BLOCK]
                * jnp.dot(own, spatial_input[b * BLOCK:(b + 1) * BLOCK], preferred_element_type=F32)
                for b in range(seq // BLOCK)
            ],
            axis=0,
        ).astype(BF16)
        for k in range(nz * ny):
            part = jnp.dot(gated, mob[k // ny, k % ny], preferred_element_type=F32).astype(BF16)
            for b in range(nx * 2):
                pm[b % 2, b // 2, :, k * cw:(k + 1) * cw] = part[b * R:(b + 1) * R]
    sc = tsem()
    send("pm", pm.at[1 - c], prc, sc, cpeer)
    with scope("mix_core"):
        arrived(prc, sc)
    for b in range(nx):
        abm[b] = (pm[c, b].astype(F32) + prc[b].astype(F32)).astype(BF16)
    sx = [tsem() for _ in range(nx)]
    for d in range(1, nx):
        send("abm", abm.at[lax.rem(x + d, nx)], pxr.at[d - 1], sx[d], xpeer(d))
    with scope("relay_gv0"):
        steps(PLAN_A)
    with scope("mix_x"):
        for d in range(1, nx):
            arrived(pxr.at[d - 1], sx[d])
    with scope("mid"):
        mix_out = pm[c, x].astype(F32) + prc[x].astype(F32)
        for d in range(1, nx):
            mix_out = mix_out + pxr[d - 1].astype(F32)
        mid[...] = (
            normalize(RESIDUAL_SCALE * tok[...].astype(F32) + mix_out) * wide(mgain)
        ).astype(BF16)
        hin[q, x, c] = normalize(mid[...].astype(F32)).astype(BF16)

    sp = tsem()
    send("hin_z", hin.at[q, x, c], hin.at[q, x, c], sp, ppeer)
    sx = [[tsem() for _ in range(nx)] for _ in range(2)]

    def rows_out(k, s):
        for d in range(1, nx):
            send("hin_x", hin.at[s, x, c], hin.at[s, x, c], sx[k][d], xpeer(d))
        send("hin_c", hin.at[s, x, c], hin.at[s, x, c], common("hin_cr"), cpeer)

    def rows_over(k, s):
        for d in range(1, nx):
            arrived(hin.at[s, xsrc(d), c], sx[k][d])
            send("hin_c", hin.at[s, xsrc(d), c], hin.at[s, xsrc(d), c], common("hin_cr"), cpeer)

    rows_out(0, q)
    with scope("relay_b"):
        steps(PLAN_B)
    with scope("rows_x0"):
        rows_over(0, q)
    with scope("relay_c"):
        steps(PLAN_C)
    with scope("pair_rows"):
        arrived(hin.at[1 - q, x, c], sp)
    rows_out(1, 1 - q)
    with scope("relay_d"):
        steps(PLAN_D)
    with scope("rows_x1"):
        rows_over(1, 1 - q)
    with scope("rows_core"):
        arrived(hin.at[:, :, 1 - c], common("hin_cr"))
    def gate_value(a):
        lhs_rows = (hin[s].reshape(seq, D) for s in range(2))
        if a < tiles:
            weights = gvb[a].reshape(D, 2 * LANES)
            tap = taps[:, pl.ds(pl.multiple_of(q * F + a * LANES, LANES), LANES)].astype(F32)
            n, at = LANES, LANES
        else:
            weights = gtb[...].reshape(D, MW)
            tap = taps[:, 2 * F:2 * F + 2 * rem].astype(F32)
            tap = jnp.where(q == 0, tap[:, :rem], tap[:, rem:])
            n, at = rem, MW // 2
        for s, lhs in enumerate(lhs_rows):
            both = jnp.dot(lhs, weights, preferred_element_type=F32)
            gate, value = both[:, :n], both[:, at:at + n]
            row = lax.broadcasted_iota(jnp.int32, gate.shape, 0)
            one = jnp.where(row >= 1, pltpu.roll(gate, 1, 0), 0.0)
            two = jnp.where(row >= 2, pltpu.roll(gate, 2, 0), 0.0)
            conv = tap[0:1] * two + tap[1:2] * one + tap[2:3] * gate
            hid[s, :, a * LANES:a * LANES + n] = (jax.nn.silu(conv) * value).astype(BF16)

    for a in range(DN):
        with scope(f"complete_gv{a}"):
            for e in range(1, ny):
                whole = gvb.at[a, :, ysrc(e)] if a < tiles else gtb.at[:, ysrc(e)]
                arrived(whole, gvy.at[a, e])
        with scope(f"gate_value{a}"):
            gate_value(a)
        with scope("relay_e"):
            steps(PLAN_E.get(a if a < tiles else TILES, ()))

    groups = sorted(
        ((i, g) for i in range(nz) for g in range(len(subs))),
        key=lambda j: (j[0] >= nz // 2, j[1] > 0 and j[0] >= nz // 2, j),
    )
    sc = {j: [tsem() for _ in range(2)] for j in groups}
    sx = {j: [[tsem() for _ in range(nx)] for _ in range(2)] for j in groups}
    turns = (1 - q, q)
    split = len(subs) > 1

    def down(item):
        (i, g), k = item
        s, zz = turns[k], source(i)[1]
        for n, e in enumerate(subs[g]):
            yy = lax.rem(y + e, ny) if split else e
            part = jnp.dot(hid[s], dnb[zz, yy], preferred_element_type=F32).astype(BF16)
            for b in range(nx * 2):
                pb[b % 2, i, g, s, b // 2, :, n * cw:(n + 1) * cw] = part[b * R:(b + 1) * R]
        send("pb", pb.at[1 - c, i, g, s], rb.at[i, g, s], sc[i, g][k], cpeer)
        crossed.append(item)

    def over_x(item):
        (i, g), k = item
        s = turns[k]
        arrived(rb.at[i, g, s], sc[i, g][k])
        for b in range(nx):
            ab[i, g, s, b] = (pb[c, i, g, s, b].astype(F32) + rb[i, g, s, b].astype(F32)).astype(BF16)
        for d in range(1, nx):
            send("ab", ab.at[i, g, s, lax.rem(x + d, nx)], xr.at[i, g, d - 1, s], sx[i, g][k][d], xpeer(d))

    def over_z(item):
        (i, g), k = item
        s, zz = turns[k], source(i)[1]
        gg = lax.rem(y + subs[g][0], ny) if split else 0
        for d in range(1, nx):
            arrived(xr.at[i, g, d - 1, s], sx[i, g][k][d])
        acc = ab[i, g, s, x].astype(F32)
        for d in range(1, nx):
            acc = acc + xr[i, g, d - 1, s].astype(F32)
        zb[zz, gg, s] = acc.astype(BF16)
        if k == 0:
            send("zb", zb.at[zz, gg, s], zr.at[zz, gg], common("zbr"), ppeer)

    crossed, summed_up = [], []
    def flush(keep_x, keep_z):
        while len(crossed) > keep_x:
            j = crossed.pop(0)
            over_x(j)
            summed_up.append(j)
        while len(summed_up) > keep_z:
            over_z(summed_up.pop(0))

    def complete_dn(j):
        i, g = j
        with scope(f"complete_dn{i}{g}"):
            for e in range(1, ny):
                if (split and e in subs[g]) or not split:
                    b = ny - e if split else e
                    d, zz = source(i)
                    arrived(dnb.at[zz, ysrc(b)], dnr.at[dn_pieces + b - 1, d])

    for j in groups:
        complete_dn(j)
        with scope(f"down{j[0]}{j[1]}"):
            down((j, 0))
            down((j, 1))
        with scope(f"relay_h{j[0]}"):
            steps(PLAN_H.get(j, ()) if split else PLAN_H.get((j[0], 0), ()) + PLAN_H.get((j[0], 1), ()))
        with scope(f"flush{j[0]}{j[1]}"):
            flush(KEEP_X, KEEP_Z)
    with scope("tail_x"):
        flush(0, 0)
    with scope("tail_z"):
        arrived(zr, common("zbr"))
    with scope("final"):
        ffn_out = jnp.concatenate(
            [zb[zz, gg, q].astype(F32) + zr[zz, gg].astype(F32) for zz in range(nz) for gg in range(len(subs))],
            axis=1,
        )
        out[...] = (
            normalize(RESIDUAL_SCALE * mid[...].astype(F32) + ffn_out) * wide(ogain)
        ).astype(BF16)
    with scope("drain_end"):
        sent("gs_z", gsb.at[pl.ds(0, nz - 1), y])
        sent("mo_z", mob.at[pl.ds(0, nz - 1)])
        far = pl.ds(0, nz - 1)
        sent("gv_z", gvb.at[:, far, y])
        sent("gt_z", gtb.at[far, y])
        sent("dn_z", dnb.at[far, y])
        over_y = pl.ds(0, ny - 1)
        sent("mo_y", mob.at[z, over_y])
        sent("gs_y", gsb.at[:, over_y])
        sent("gv_y", gvb.at[:, :, over_y])
        sent("gt_y", gtb.at[:, over_y])
        sent("dn_y", dnb.at[:, over_y])
        sent("xin_x", xin.at[pl.ds(0, nx - 1), 0])
        sent("xin_c", xin.at[:, c])
        sent("stat", stat.at[pl.ds(0, 2 * nx - 1)])
        sent("pm", prc)
        sent("abm", pxr)
        sent("hin_z", hin.at[q, x, c])
        sent("hin_x", hin.at[:, pl.ds(0, nx - 1), c])
        sent("hin_c", hin.at[:, :, c])
        sent("pb", rb)
        sent("ab", xr)
        sent("zb", zr)


def shards(nf, nt, ny, tokens, gate_proj, signal_proj, spatial, signal_gain, mixer_out, mixer_gain, ffn_gate, ffn_value, conv_taps, ffn_down, output_gain):
    nz = nf // ny
    nx = nt // 2
    R, D = tokens.shape
    K, C = gate_proj.shape
    H = ffn_gate.shape[1]
    full = H // (2 * LANES) * LANES
    rem = H // 2 - full
    W = full + rem
    MW = -(-2 * rem // LANES) * LANES
    cw = mixer_out.shape[1]
    seq = nx * 2 * R
    subs = [(e,) for e in range(ny)] if cw % LANES == 0 else [tuple(range(ny))]
    gw = cw * len(subs[0])
    ns = len(subs)
    dn_pieces = DN_PIECES
    packed = bool(C % LANES or (2 * rem) % LANES)
    if packed:
        gp = jnp.concatenate([gate_proj, signal_proj], axis=1)
        gt, vt = ffn_gate[:, 2 * full:], ffn_value[:, 2 * full:]
    else:
        gp, gt, vt = gate_proj, ffn_gate, ffn_value

    vm = pltpu.VMEM
    dma = pltpu.SemaphoreType.DMA
    n_t = 6 * nx + 2 + nz * ns * (2 + 2 * nx)
    scratch = [
        vm((nz, ny, K, 2 * C), BF16),
        vm((nz, ny) + mixer_out.shape, BF16),
        vm((full // LANES, nz, ny, K, 2 * LANES), BF16),
        vm((nz, ny, K, MW), BF16),
        vm((nz, ny, W, cw), BF16),
        vm((2, K, 2 * rem), BF16),
        vm((2, K, MW), BF16),
        vm((nx, 2, R, D), BF16),
        vm((2 * nx, 8, seq), F32),
        vm((2, nx, R, D), BF16),
        vm((nx, R, D), BF16),
        vm((nx, R, D), BF16),
        vm((nx - 1, R, D), BF16),
        vm((R, D), BF16),
        vm((2, nx, 2, R, D), BF16),
        vm((2, seq, W), BF16),
        vm((2, nz, ns, 2, nx, R, gw), BF16),
        vm((nz, ns, 2, nx, R, gw), BF16),
        vm((nz, ns, 2, nx, R, gw), BF16),
        vm((nz, ns, nx - 1, 2, R, gw), BF16),
        vm((nz, ns, 2, R, gw), BF16),
        vm((nz, ns, R, gw), BF16),
        dma((5,)),
        dma((nz,)),
        dma((nz,)),
        dma((full // LANES + 1, nz)),
        dma((full // LANES + 1, ny)),
        dma((dn_pieces + ny - 1, nz)),
        dma((24 + 2 * (ny - 1),)),
        dma((n_t,)),
    ]
    here, there = pl.BlockSpec(memory_space=pltpu.VMEM), pl.BlockSpec(memory_space=pl.ANY)
    return pl.pallas_call(
        functools.partial(kernel, nz, ny, nx, full, rem, subs, packed, dn_pieces),
        out_shape=jax.ShapeDtypeStruct((R, D), BF16),
        in_specs=[here] + [there] * 8 + [here] * 5,
        out_specs=here,
        scratch_shapes=scratch,
        compiler_params=pltpu.CompilerParams(
            collective_id=0, has_side_effects=True, vmem_limit_bytes=67043328
        ),
    )(
        tokens, gp, signal_proj, mixer_out, ffn_gate, ffn_value, gt, vt, ffn_down, spatial,
        signal_gain, mixer_gain, conv_taps, output_gain,
    )


def solution(mesh):
    nf, nt = mesh.shape["fs"], mesh.shape["tp"]
    ny = 2 ** (int(math.log2(nf // 2)) // 2)
    in_specs = (
        P(("fs", "tp"), None),
        P("fs", "tp"),
        P("fs", "tp"),
        P(),
        P("tp"),
        P("tp", "fs"),
        P(),
        P("fs", "tp"),
        P("fs", "tp"),
        P(None, "tp"),
        P("tp", "fs"),
        P(),
    )
    return jax.shard_map(
        functools.partial(shards, nf, nt, ny),
        mesh=mesh,
        in_specs=in_specs,
        out_specs=P(("fs", "tp"), None),
        check_vma=False,
    )
```

```python
import functools
import math

import jax
import jax.numpy as jnp
from jax import lax
from jax.experimental import pallas as pl
from jax.experimental.pallas import tpu as pltpu
from jax.sharding import PartitionSpec as P

MIX_WIDTH = 512
HEAD_SIZE = 128
BLOCK = 128
SEGMENT = 64
LANES = 128
TILES = 5
DN_PIECES = 2
KEEP_X, KEEP_Z = 0, 4
EPSILON = 1e-05
RESIDUAL_SCALE = math.sqrt(2.0)
MESH = pl.DeviceIdType.MESH
F32 = jnp.float32
BF16 = jnp.bfloat16


def normalize(values):
    row_mean = jnp.mean(values, axis=-1, keepdims=True)
    centred = values - row_mean
    spread = jnp.mean(centred * centred, axis=-1, keepdims=True)
    return centred * lax.rsqrt(spread + EPSILON)


def wide(gain):
    return gain[...].astype(F32)[None]


def plan(*words):
    return tuple(
        (w[0], int(w[1], 16), d) for w in words for d in ((1, 2, 3) if w[2] == "*" else (int(w[2]),))
    )


PLAN_Y0 = plan("o00")
PLAN_Y = plan("o10", "o20", "o30", "o40", "o50", "o60", "o70")
PLAN_FIRST = plan()
PLAN_M0 = plan("m00", "m10", "m20")
PLAN_M = plan()
PLAN_0 = plan("i01", "i02", "w00", "i11", "i12", "w10", "i22", "w20", "i21")
PLAN_A = plan("r01", "r02", "r03", "r11", "n30")
PLAN_B = plan("i31", "n40", "i41", "n50", "i51", "r12", "r21", "r13", "r22", "r23")
PLAN_C = plan("e30", "r31")
PLAN_D = plan("e40", "r41", "e50", "n60", "r51", "i61", "r32", "e60", "r33", "i71", "n70", "r42", "r43", "e70", "r52", "r53")
PLAN_E = {1: plan("r61"), 4: plan("r71")}
PLAN_H = {(0, 0): plan("r62"), (0, 1): plan("r63"), (1, 0): plan(), (1, 1): plan("r72", "r73")}


def kernel(
    nz, ny, nx, full, rem, subs, packed, dn_pieces,
    tok, gp, sp_, mo, fg, fv, gt, vt, dn, spatial, sgain, mgain, taps, ogain,
    out,
    gsb, mob, gvb, gtb, dnb, tails, mixed, xin, stat, pm, prc, abm, pxr, mid, hin, hid, pb, rb, ab, xr, zb, zr,
    loc_sem, gzr, mzr, gvr, gvy, dnr, shared, ts,
):
    R, D = tok.shape
    C, cw = mo.shape
    K = fg.shape[0]
    F = full
    W = full + rem
    MW = mixed.shape[2]
    f = lax.axis_index("fs")
    t = lax.axis_index("tp")
    z, y = f // ny, f % ny
    x, c = t // 2, t % 2
    q = z % 2
    seq = nx * 2 * R
    gw = ny * cw

    def zsrc(d):
        zz = z
        for bit in (1 << k for k in range(d.bit_length())):
            if d & bit:
                zz = zz + bit - 2 * bit * ((z // bit) % 2)
        return zz

    def zpeer(d):
        return (zsrc(d) * ny + y, t)

    inner = ((z + 1) // 2) % 2

    def source(k):
        if nz != 4 or k < 2:
            return k, zsrc(k)
        return (3 - inner, 3 - 3 * (z // 2)) if k == 2 else (2 + inner, 2 - z // 2)

    def ypeer(e):
        return (z * ny + lax.rem(y + e, ny), t)

    def xpeer(d):
        return (f, lax.rem(x + d, nx) * 2 + c)

    def tpeer(d, e):
        return (f, lax.rem(x + d, nx) * 2 + (c if e == 0 else 1 - c))

    cpeer = (f, x * 2 + 1 - c)
    ppeer = ((z + 1 - 2 * q) * ny + y, t)

    def ysrc(e):
        return lax.rem(y + ny - e, ny)

    def xsrc(d):
        return lax.rem(x + nx - d, nx)

    names = {}

    def common(name):
        return shared.at[names.setdefault(name, len(names))]

    def remote(src, dst, ssem, rsem, to):
        return pltpu.make_async_remote_copy(
            src_ref=src, dst_ref=dst, send_sem=ssem, recv_sem=rsem, device_id=to, device_id_type=MESH
        )

    def send(kind, src, dst, rsem, to):
        remote(src, dst, common(kind), rsem, to).start()

    def arrived(dst, rsem):
        pltpu.make_async_copy(dst, dst, rsem).wait()

    def sent(kind, whole):
        pltpu.make_async_copy(whole, whole, common(kind)).wait()

    scope = jax.named_scope
    tslot = [0]

    def tsem():
        k = tslot[0]
        tslot[0] += 1
        return ts.at[k]

    dn_rows = W // dn_pieces
    tiles = F // LANES
    DN = tiles + 1

    def parts(a, h, zz, yy):
        if a < tiles:
            at = pl.ds(pl.multiple_of(h * F + a * LANES, LANES), LANES)
            dst = gvb.at[a, zz, yy]
            return [(fg.at[:, at], dst.at[:, pl.ds(0, LANES)]), (fv.at[:, at], dst.at[:, pl.ds(LANES, LANES)])]
        if a < DN:
            return [(mixed.at[h], gtb.at[zz, yy])]
        lo, hi = (a - DN) * dn_rows, (a - DN + 1) * dn_rows
        dst = dnb.at[zz, yy]
        found = []
        if lo < F:
            n = min(hi, F) - lo
            found.append((dn.at[pl.ds(pl.multiple_of(h * F + lo, 16), n)], dst.at[pl.ds(lo, n)]))
        if hi > F:
            s = max(lo, F)
            n = hi - s
            found.append(
                (dn.at[pl.ds(pl.multiple_of(2 * F + h * rem + s - F, 16), n)], dst.at[pl.ds(s, n)])
            )
        return found

    def slot(a, zz, yy):
        if a < tiles:
            return gvb.at[a, zz, yy]
        if a < DN:
            return gtb.at[zz, yy]
        return dnb.at[zz, yy, pl.ds((a - DN) * dn_rows, dn_rows)]

    def fetch(k, src, dst):
        pltpu.make_async_copy(src, dst, loc_sem.at[k]).start()

    def ready(k, whole):
        pltpu.make_async_copy(whole, whole, loc_sem.at[k]).wait()

    GS, MO, TAILS, GV, DOWN = range(5)
    if packed:
        fetch(GS, gp, gsb.at[z, y])
    else:
        fetch(GS, gp, gsb.at[z, y, :, pl.ds(0, C)])
        fetch(GS, sp_, gsb.at[z, y, :, pl.ds(C, C)])
    fetch(MO, mo, mob.at[z, y])
    T = tails.shape[2]
    if packed:
        fetch(TAILS, gt, tails.at[0])
        fetch(TAILS, vt, tails.at[1])
    else:
        fetch(TAILS, gt.at[:, pl.ds(2 * F, T)], tails.at[0])
        fetch(TAILS, vt.at[:, pl.ds(2 * F, T)], tails.at[1])
    for a in range(tiles):
        for src, dst in parts(a, q, z, y):
            fetch(GV, src, dst)
    for a in range(DN, DN + dn_pieces):
        for src, dst in parts(a, q, z, y):
            fetch(DOWN, src, dst)

    barrier = pltpu.get_barrier_semaphore()
    peers = [zpeer(d) for d in range(1, nz)] + [ypeer(e) for e in range(1, ny)]
    peers += [tpeer(d, e) for d in range(nx) for e in range(2) if d + e]
    for p in peers:
        pl.semaphore_signal(barrier, inc=1, device_id=p, device_id_type=MESH)

    ready(TAILS, tails)
    for h in range(2):
        for k in range(2):
            mixed[h, :, k * (MW // 2):k * (MW // 2) + rem] = tails[k, :, h * rem:(h + 1) * rem]
    for k in range(2):
        part = tails[k].astype(F32)
        part = jnp.where(q == 0, part[:, :rem], part[:, rem:2 * rem]).astype(BF16)
        gtb[z, y, :, k * (MW // 2):k * (MW // 2) + rem] = part
    ready(GS, gsb.at[z, y])
    ready(MO, mob.at[z, y])
    pl.semaphore_wait(barrier, len(peers))

    def issue_z(a, d):
        for src, dst in parts(a, zsrc(d) % 2, z, y):
            remote(src, dst, common(family(a) + "_z"), z_sem(a, d), zpeer(d)).start()

    def z_sem(a, d):
        return gvr.at[a, d] if a < DN else dnr.at[a - DN, d]

    def y_sem(a, d, e):
        return gvy.at[a, e] if a < DN else dnr.at[dn_pieces + e - 1, d]

    def family(a):
        return "gv" if a < tiles else "gt" if a < DN else "dn"

    def issue_y(a):
        for e in range(1, ny):
            send(family(a) + "_y", slot(a, z, y), slot(a, z, y), y_sem(a, 0, e), ypeer(e))

    def relay(a, k):
        d, zz = source(k)
        arrived(slot(a, zz, y), z_sem(a, d))
        for e in range(1, ny):
            send(family(a) + "_y", slot(a, zz, y), slot(a, zz, y), y_sem(a, d, e), ypeer(e))

    bits = [1 << k for k in reversed(range((nz - 1).bit_length()))]

    def spread(kind, buf, d, rsem):
        src = zsrc(d)
        for bit in bits:
            if d == 0 or bit < (d & -d):
                send(kind, buf(src), buf(src), rsem.at[d | bit], zpeer(bit))

    def issue_far(a, what):
        if nz != 4:
            for d in range(2, nz):
                if (what == "n") == (d == 2) and what != "w" and (what != "m" or d > 2):
                    issue_z(a, d)
            return
        if what in "mw":
            pl.when(inner == (1 if what == "m" else 0))(lambda: issue_z(a, 3))
            return
        row = 2 - z // 2 if what == "n" else 3 - 3 * (z // 2)
        d = 2 + inner if what == "n" else 3 - inner
        for src, dst in parts(a, row % 2, z, y):
            remote(src, dst, common(family(a) + "_z"), z_sem(a, d), (row * ny + y, t)).start()

    def steps(plan):
        for what, piece, d in plan:
            if piece < TILES and piece >= tiles:
                continue
            a = piece if piece < TILES else piece - TILES + tiles
            if what == "o":
                issue_y(a)
            elif what in "nemw":
                issue_far(a, what)
            for dd in range(1, nz):
                if dd == d or (d == 3 and dd > 3):
                    (relay if what == "r" else issue_z)(a, dd)

    def gs_block(src):
        return gsb.at[src, y]

    def mo_block(src):
        return mob.at[src]

    spread("gs_z", gs_block, 0, gzr)
    for e in range(1, ny):
        send("mo_y", mob.at[z, y], mob.at[z, y], common(f"mo_y{e}r"), ypeer(e))
    for e in range(1, ny):
        send("gs_y", gsb.at[z, y], gsb.at[z, y], common(f"gs_y{e}r"), ypeer(e))
    ready(GV, gvb.at[:, z, y])
    steps(PLAN_Y0)
    steps(PLAN_FIRST)

    xin[x, c] = normalize(tok[...].astype(F32)).astype(BF16)
    s1 = [tsem() for _ in range(nx)]
    for d in range(1, nx):
        send("xin_x", xin.at[x, c], xin.at[x, c], s1[d], xpeer(d))
    send("xin_c", xin.at[x, c], xin.at[x, c], common("xin_cr"), cpeer)

    with scope("mo_y"):
        for e in range(1, ny):
            arrived(mob.at[z, ysrc(e)], common(f"mo_y{e}r"))
    spread("mo_z", mo_block, 0, mzr)
    steps(PLAN_M0)
    for d in range(1, nz):
        with scope(f"relay_gs{d}"):
            arrived(gs_block(zsrc(d)), gzr.at[d])
            spread("gs_z", gs_block, d, gzr)
            for e in range(1, ny):
                send("gs_y", gs_block(zsrc(d)), gs_block(zsrc(d)), common(f"gs_y{e}r"), ypeer(e))
    steps(PLAN_M)
    for d in range(1, nz):
        with scope(f"relay_mo{d}"):
            arrived(mo_block(zsrc(d)), mzr.at[d])
            spread("mo_z", mo_block, d, mzr)
    with scope("first_z"):
        steps(PLAN_0)
    ready(DOWN, dnb.at[z, y])
    steps(PLAN_Y)
    with scope("xin"):
        for d in range(1, nx):
            arrived(xin.at[xsrc(d), c], s1[d])
            send("xin_c", xin.at[xsrc(d), c], xin.at[xsrc(d), c], common("xin_cr"), cpeer)
        arrived(xin.at[:, 1 - c], common("xin_cr"))
    with scope("complete_gs"):
        for e in range(1, ny):
            arrived(gsb.at[:, ysrc(e)], common(f"gs_y{e}r"))

    with scope("mix_in"):
        pre = jnp.dot(xin[...].reshape(seq, D), gsb[...].reshape(D, 2 * C), preferred_element_type=F32)
        branch_signal = jax.nn.gelu(pre[:, C:])
        total = jnp.sum(branch_signal, axis=1, keepdims=True)
        square = jnp.sum(branch_signal * branch_signal, axis=1, keepdims=True)
        lane = lax.broadcasted_iota(jnp.int32, (seq, LANES), 1)
        stat[0] = jnp.where(lane == 0, total, square).T[:8]
    others = [(d, e) for d in range(nx) for e in range(2) if d + e]
    sx = {}
    for d, e in others:
        sx[d, e] = tsem()
        send("stat", stat.at[0], stat.at[2 * d + e], sx[d, e], tpeer(d, e))
    branch_gate = jax.nn.gelu(pre[:, :C])
    with scope("stats"):
        summed = stat[0]
        for d, e in others:
            arrived(stat.at[2 * d + e], sx[d, e])
            summed = summed + stat[2 * d + e]
    with scope("mix_out"):
        back = summed.T
        row_mean = back[:, 0:1] / MIX_WIDTH
        spread = back[:, 1:2] / MIX_WIDTH - row_mean * row_mean
        spatial_input = (
            (branch_signal - row_mean) * lax.rsqrt(spread + EPSILON) * wide(sgain)
        ).astype(BF16)
        rows_i = lax.broadcasted_iota(jnp.int32, (BLOCK, BLOCK), 0) // SEGMENT
        cols_i = lax.broadcasted_iota(jnp.int32, (BLOCK, BLOCK), 1) // SEGMENT
        own = spatial[t * C // HEAD_SIZE]
        own = jnp.where(cols_i <= rows_i, own, jnp.zeros_like(own))
        gated = jnp.concatenate(
            [
                branch_gate[b * BLOCK:(b + 1) * BLOCK]
                * jnp.dot(own, spatial_input[b * BLOCK:(b + 1) * BLOCK], preferred_element_type=F32)
                for b in range(seq // BLOCK)
            ],
            axis=0,
        ).astype(BF16)
        for k in range(nz * ny):
            part = jnp.dot(gated, mob[k // ny, k % ny], preferred_element_type=F32).astype(BF16)
            for b in range(nx * 2):
                pm[b % 2, b // 2, :, k * cw:(k + 1) * cw] = part[b * R:(b + 1) * R]
    sc = tsem()
    send("pm", pm.at[1 - c], prc, sc, cpeer)
    with scope("mix_core"):
        arrived(prc, sc)
    for b in range(nx):
        abm[b] = (pm[c, b].astype(F32) + prc[b].astype(F32)).astype(BF16)
    sx = [tsem() for _ in range(nx)]
    for d in range(1, nx):
        send("abm", abm.at[lax.rem(x + d, nx)], pxr.at[d - 1], sx[d], xpeer(d))
    with scope("relay_gv0"):
        steps(PLAN_A)
    with scope("mix_x"):
        for d in range(1, nx):
            arrived(pxr.at[d - 1], sx[d])
    with scope("mid"):
        mix_out = pm[c, x].astype(F32) + prc[x].astype(F32)
        for d in range(1, nx):
            mix_out = mix_out + pxr[d - 1].astype(F32)
        mid[...] = (
            normalize(RESIDUAL_SCALE * tok[...].astype(F32) + mix_out) * wide(mgain)
        ).astype(BF16)
        hin[q, x, c] = normalize(mid[...].astype(F32)).astype(BF16)

    sp = tsem()
    send("hin_z", hin.at[q, x, c], hin.at[q, x, c], sp, ppeer)
    sx = [[tsem() for _ in range(nx)] for _ in range(2)]

    def rows_out(k, s):
        for d in range(1, nx):
            send("hin_x", hin.at[s, x, c], hin.at[s, x, c], sx[k][d], xpeer(d))
        send("hin_c", hin.at[s, x, c], hin.at[s, x, c], common("hin_cr"), cpeer)

    def rows_over(k, s):
        for d in range(1, nx):
            arrived(hin.at[s, xsrc(d), c], sx[k][d])
            send("hin_c", hin.at[s, xsrc(d), c], hin.at[s, xsrc(d), c], common("hin_cr"), cpeer)

    rows_out(0, q)
    with scope("relay_b"):
        steps(PLAN_B)
    with scope("rows_x0"):
        rows_over(0, q)
    with scope("relay_c"):
        steps(PLAN_C)
    with scope("pair_rows"):
        arrived(hin.at[1 - q, x, c], sp)
    rows_out(1, 1 - q)
    with scope("relay_d"):
        steps(PLAN_D)
    with scope("rows_x1"):
        rows_over(1, 1 - q)
    with scope("rows_core"):
        arrived(hin.at[:, :, 1 - c], common("hin_cr"))
    def gate_value(a):
        lhs_rows = (hin[s].reshape(seq, D) for s in range(2))
        if a < tiles:
            weights = gvb[a].reshape(D, 2 * LANES)
            tap = taps[:, pl.ds(pl.multiple_of(q * F + a * LANES, LANES), LANES)].astype(F32)
            n, at = LANES, LANES
        else:
            weights = gtb[...].reshape(D, MW)
            tap = taps[:, 2 * F:2 * F + 2 * rem].astype(F32)
            tap = jnp.where(q == 0, tap[:, :rem], tap[:, rem:])
            n, at = rem, MW // 2
        for s, lhs in enumerate(lhs_rows):
            both = jnp.dot(lhs, weights, preferred_element_type=F32)
            gate, value = both[:, :n], both[:, at:at + n]
            row = lax.broadcasted_iota(jnp.int32, gate.shape, 0)
            one = jnp.where(row >= 1, pltpu.roll(gate, 1, 0), 0.0)
            two = jnp.where(row >= 2, pltpu.roll(gate, 2, 0), 0.0)
            conv = tap[0:1] * two + tap[1:2] * one + tap[2:3] * gate
            hid[s, :, a * LANES:a * LANES + n] = (jax.nn.silu(conv) * value).astype(BF16)

    for a in range(DN):
        with scope(f"complete_gv{a}"):
            for e in range(1, ny):
                whole = gvb.at[a, :, ysrc(e)] if a < tiles else gtb.at[:, ysrc(e)]
                arrived(whole, gvy.at[a, e])
        with scope(f"gate_value{a}"):
            gate_value(a)
        with scope("relay_e"):
            steps(PLAN_E.get(a if a < tiles else TILES, ()))

    groups = sorted(
        ((i, g) for i in range(nz) for g in range(len(subs))),
        key=lambda j: (j[0] >= nz // 2, j[1] > 0 and j[0] >= nz // 2, j),
    )
    sc = {j: [tsem() for _ in range(2)] for j in groups}
    sx = {j: [[tsem() for _ in range(nx)] for _ in range(2)] for j in groups}
    turns = (1 - q, q)
    split = len(subs) > 1

    def down(item):
        (i, g), k = item
        s, zz = turns[k], source(i)[1]
        for n, e in enumerate(subs[g]):
            yy = lax.rem(y + e, ny) if split else e
            part = jnp.dot(hid[s], dnb[zz, yy], preferred_element_type=F32).astype(BF16)
            for b in range(nx * 2):
                pb[b % 2, i, g, s, b // 2, :, n * cw:(n + 1) * cw] = part[b * R:(b + 1) * R]
        send("pb", pb.at[1 - c, i, g, s], rb.at[i, g, s], sc[i, g][k], cpeer)
        crossed.append(item)

    def over_x(item):
        (i, g), k = item
        s = turns[k]
        arrived(rb.at[i, g, s], sc[i, g][k])
        for b in range(nx):
            ab[i, g, s, b] = (pb[c, i, g, s, b].astype(F32) + rb[i, g, s, b].astype(F32)).astype(BF16)
        for d in range(1, nx):
            send("ab", ab.at[i, g, s, lax.rem(x + d, nx)], xr.at[i, g, d - 1, s], sx[i, g][k][d], xpeer(d))

    def over_z(item):
        (i, g), k = item
        s, zz = turns[k], source(i)[1]
        gg = lax.rem(y + subs[g][0], ny) if split else 0
        for d in range(1, nx):
            arrived(xr.at[i, g, d - 1, s], sx[i, g][k][d])
        acc = ab[i, g, s, x].astype(F32)
        for d in range(1, nx):
            acc = acc + xr[i, g, d - 1, s].astype(F32)
        zb[zz, gg, s] = acc.astype(BF16)
        if k == 0:
            send("zb", zb.at[zz, gg, s], zr.at[zz, gg], common("zbr"), ppeer)

    crossed, summed_up = [], []
    def flush(keep_x, keep_z):
        while len(crossed) > keep_x:
            j = crossed.pop(0)
            over_x(j)
            summed_up.append(j)
        while len(summed_up) > keep_z:
            over_z(summed_up.pop(0))

    def complete_dn(j):
        i, g = j
        with scope(f"complete_dn{i}{g}"):
            for e in range(1, ny):
                if (split and e in subs[g]) or not split:
                    b = ny - e if split else e
                    d, zz = source(i)
                    arrived(dnb.at[zz, ysrc(b)], dnr.at[dn_pieces + b - 1, d])

    for j in groups:
        complete_dn(j)
        with scope(f"down{j[0]}{j[1]}"):
            down((j, 0))
            down((j, 1))
        with scope(f"relay_h{j[0]}"):
            steps(PLAN_H.get(j, ()) if split else PLAN_H.get((j[0], 0), ()) + PLAN_H.get((j[0], 1), ()))
        with scope(f"flush{j[0]}{j[1]}"):
            flush(KEEP_X, KEEP_Z)
    with scope("tail_x"):
        flush(0, 0)
    with scope("tail_z"):
        arrived(zr, common("zbr"))
    with scope("final"):
        ffn_out = jnp.concatenate(
            [zb[zz, gg, q].astype(F32) + zr[zz, gg].astype(F32) for zz in range(nz) for gg in range(len(subs))],
            axis=1,
        )
        out[...] = (
            normalize(RESIDUAL_SCALE * mid[...].astype(F32) + ffn_out) * wide(ogain)
        ).astype(BF16)
    with scope("drain_end"):
        sent("gs_z", gsb.at[pl.ds(0, nz - 1), y])
        sent("mo_z", mob.at[pl.ds(0, nz - 1)])
        far = pl.ds(0, nz - 1)
        sent("gv_z", gvb.at[:, far, y])
        sent("gt_z", gtb.at[far, y])
        sent("dn_z", dnb.at[far, y])
        over_y = pl.ds(0, ny - 1)
        sent("mo_y", mob.at[z, over_y])
        sent("gs_y", gsb.at[:, over_y])
        sent("gv_y", gvb.at[:, :, over_y])
        sent("gt_y", gtb.at[:, over_y])
        sent("dn_y", dnb.at[:, over_y])
        sent("xin_x", xin.at[pl.ds(0, nx - 1), 0])
        sent("xin_c", xin.at[:, c])
        sent("stat", stat.at[pl.ds(0, 2 * nx - 1)])
        sent("pm", prc)
        sent("abm", pxr)
        sent("hin_z", hin.at[q, x, c])
        sent("hin_x", hin.at[:, pl.ds(0, nx - 1), c])
        sent("hin_c", hin.at[:, :, c])
        sent("pb", rb)
        sent("ab", xr)
        sent("zb", zr)


def shards(nf, nt, ny, tokens, gate_proj, signal_proj, spatial, signal_gain, mixer_out, mixer_gain, ffn_gate, ffn_value, conv_taps, ffn_down, output_gain):
    nz = nf // ny
    nx = nt // 2
    R, D = tokens.shape
    K, C = gate_proj.shape
    H = ffn_gate.shape[1]
    full = H // (2 * LANES) * LANES
    rem = H // 2 - full
    W = full + rem
    MW = -(-2 * rem // LANES) * LANES
    cw = mixer_out.shape[1]
    seq = nx * 2 * R
    subs = [(e,) for e in range(ny)] if cw % LANES == 0 else [tuple(range(ny))]
    gw = cw * len(subs[0])
    ns = len(subs)
    dn_pieces = DN_PIECES
    packed = bool(C % LANES or (2 * rem) % LANES)
    if packed:
        gp = jnp.concatenate([gate_proj, signal_proj], axis=1)
        gt, vt = ffn_gate[:, 2 * full:], ffn_value[:, 2 * full:]
    else:
        gp, gt, vt = gate_proj, ffn_gate, ffn_value

    vm = pltpu.VMEM
    dma = pltpu.SemaphoreType.DMA
    n_t = 6 * nx + 2 + nz * ns * (2 + 2 * nx)
    scratch = [
        vm((nz, ny, K, 2 * C), BF16),
        vm((nz, ny) + mixer_out.shape, BF16),
        vm((full // LANES, nz, ny, K, 2 * LANES), BF16),
        vm((nz, ny, K, MW), BF16),
        vm((nz, ny, W, cw), BF16),
        vm((2, K, 2 * rem), BF16),
        vm((2, K, MW), BF16),
        vm((nx, 2, R, D), BF16),
        vm((2 * nx, 8, seq), F32),
        vm((2, nx, R, D), BF16),
        vm((nx, R, D), BF16),
        vm((nx, R, D), BF16),
        vm((nx - 1, R, D), BF16),
        vm((R, D), BF16),
        vm((2, nx, 2, R, D), BF16),
        vm((2, seq, W), BF16),
        vm((2, nz, ns, 2, nx, R, gw), BF16),
        vm((nz, ns, 2, nx, R, gw), BF16),
        vm((nz, ns, 2, nx, R, gw), BF16),
        vm((nz, ns, nx - 1, 2, R, gw), BF16),
        vm((nz, ns, 2, R, gw), BF16),
        vm((nz, ns, R, gw), BF16),
        dma((5,)),
        dma((nz,)),
        dma((nz,)),
        dma((full // LANES + 1, nz)),
        dma((full // LANES + 1, ny)),
        dma((dn_pieces + ny - 1, nz)),
        dma((24 + 2 * (ny - 1),)),
        dma((n_t,)),
    ]
    here, there = pl.BlockSpec(memory_space=pltpu.VMEM), pl.BlockSpec(memory_space=pl.ANY)
    return pl.pallas_call(
        functools.partial(kernel, nz, ny, nx, full, rem, subs, packed, dn_pieces),
        out_shape=jax.ShapeDtypeStruct((R, D), BF16),
        in_specs=[here] + [there] * 8 + [here] * 5,
        out_specs=here,
        scratch_shapes=scratch,
        compiler_params=pltpu.CompilerParams(
            collective_id=0, has_side_effects=True, vmem_limit_bytes=67043328
        ),
    )(
        tokens, gp, signal_proj, mixer_out, ffn_gate, ffn_value, gt, vt, ffn_down, spatial,
        signal_gain, mixer_gain, conv_taps, output_gain,
    )


def solution(mesh):
    nf, nt = mesh.shape["fs"], mesh.shape["tp"]
    ny = 2 ** (int(math.log2(nf // 2)) // 2)
    in_specs = (
        P(("fs", "tp"), None),
        P("fs", "tp"),
        P("fs", "tp"),
        P(),
        P("tp"),
        P("tp", "fs"),
        P(),
        P("fs", "tp"),
        P("fs", "tp"),
        P(None, "tp"),
        P("tp", "fs"),
        P(),
    )
    return jax.shard_map(
        functools.partial(shards, nf, nt, ny),
        mesh=mesh,
        in_specs=in_specs,
        out_specs=P(("fs", "tp"), None),
        check_vma=False,
    )
```

```python
import functools
import math

import jax
import jax.numpy as jnp
from jax import lax
from jax.experimental import pallas as pl
from jax.experimental.pallas import tpu as pltpu
from jax.sharding import PartitionSpec as P

MIX_WIDTH = 512
HEAD_SIZE = 128
BLOCK = 128
SEGMENT = 64
LANES = 128
TILES = 5
DN_PIECES = 2
KEEP_X, KEEP_Z = 0, 4
EPSILON = 1e-05
RESIDUAL_SCALE = math.sqrt(2.0)
MESH = pl.DeviceIdType.MESH
F32 = jnp.float32
BF16 = jnp.bfloat16


def normalize(values):
    row_mean = jnp.mean(values, axis=-1, keepdims=True)
    centred = values - row_mean
    spread = jnp.mean(centred * centred, axis=-1, keepdims=True)
    return centred * lax.rsqrt(spread + EPSILON)


def wide(gain):
    return gain[...].astype(F32)[None]


def plan(*words):
    return tuple(
        (w[0], int(w[1], 16), d) for w in words for d in ((1, 2, 3) if w[2] == "*" else (int(w[2]),))
    )


PLAN_Y0 = plan("o00", "o50")
PLAN_Y = plan("o10", "o20", "o30", "o40", "o60", "o70")
PLAN_FIRST = plan()
PLAN_M0 = plan("m00", "m10", "m20")
PLAN_M = plan()
PLAN_0 = plan("i01", "i02", "w00", "i11", "i12", "w10", "i22", "w20", "i21")
PLAN_A = plan("r01", "r02", "r03", "r11", "n30")
PLAN_B = plan("i31", "n40", "i41", "n50", "i51", "r12", "r21", "r13", "r22", "r23")
PLAN_C = plan("e30", "r31")
PLAN_D = plan("e40", "r41", "e50", "n60", "r51", "i61", "r32", "e60", "r33", "i71", "n70", "r42", "r43", "e70", "r52", "r53")
PLAN_E = {1: plan("r61"), 4: plan("r71")}
PLAN_H = {(0, 0): plan("r62"), (0, 1): plan("r63"), (1, 0): plan(), (1, 1): plan("r72", "r73")}


def kernel(
    nz, ny, nx, full, rem, subs, packed, dn_pieces,
    tok, gp, sp_, mo, fg, fv, gt, vt, dn, spatial, sgain, mgain, taps, ogain,
    out,
    gsb, mob, gvb, gtb, dnb, tails, mixed, xin, stat, pm, prc, abm, pxr, mid, hin, hid, pb, rb, ab, xr, zb, zr,
    loc_sem, gzr, mzr, gvr, gvy, dnr, shared, ts,
):
    R, D = tok.shape
    C, cw = mo.shape
    K = fg.shape[0]
    F = full
    W = full + rem
    MW = mixed.shape[2]
    f = lax.axis_index("fs")
    t = lax.axis_index("tp")
    z, y = f // ny, f % ny
    x, c = t // 2, t % 2
    q = z % 2
    seq = nx * 2 * R
    gw = ny * cw

    def zsrc(d):
        zz = z
        for bit in (1 << k for k in range(d.bit_length())):
            if d & bit:
                zz = zz + bit - 2 * bit * ((z // bit) % 2)
        return zz

    def zpeer(d):
        return (zsrc(d) * ny + y, t)

    inner = ((z + 1) // 2) % 2

    def source(k):
        if nz != 4 or k < 2:
            return k, zsrc(k)
        return (3 - inner, 3 - 3 * (z // 2)) if k == 2 else (2 + inner, 2 - z // 2)

    def ypeer(e):
        return (z * ny + lax.rem(y + e, ny), t)

    def xpeer(d):
        return (f, lax.rem(x + d, nx) * 2 + c)

    def tpeer(d, e):
        return (f, lax.rem(x + d, nx) * 2 + (c if e == 0 else 1 - c))

    cpeer = (f, x * 2 + 1 - c)
    ppeer = ((z + 1 - 2 * q) * ny + y, t)

    def ysrc(e):
        return lax.rem(y + ny - e, ny)

    def xsrc(d):
        return lax.rem(x + nx - d, nx)

    names = {}

    def common(name):
        return shared.at[names.setdefault(name, len(names))]

    def remote(src, dst, ssem, rsem, to):
        return pltpu.make_async_remote_copy(
            src_ref=src, dst_ref=dst, send_sem=ssem, recv_sem=rsem, device_id=to, device_id_type=MESH
        )

    def send(kind, src, dst, rsem, to):
        remote(src, dst, common(kind), rsem, to).start()

    def arrived(dst, rsem):
        pltpu.make_async_copy(dst, dst, rsem).wait()

    def sent(kind, whole):
        pltpu.make_async_copy(whole, whole, common(kind)).wait()

    scope = jax.named_scope
    tslot = [0]

    def tsem():
        k = tslot[0]
        tslot[0] += 1
        return ts.at[k]

    dn_rows = W // dn_pieces
    tiles = F // LANES
    DN = tiles + 1

    def parts(a, h, zz, yy):
        if a < tiles:
            at = pl.ds(pl.multiple_of(h * F + a * LANES, LANES), LANES)
            dst = gvb.at[a, zz, yy]
            return [(fg.at[:, at], dst.at[:, pl.ds(0, LANES)]), (fv.at[:, at], dst.at[:, pl.ds(LANES, LANES)])]
        if a < DN:
            return [(mixed.at[h], gtb.at[zz, yy])]
        lo, hi = (a - DN) * dn_rows, (a - DN + 1) * dn_rows
        dst = dnb.at[zz, yy]
        found = []
        if lo < F:
            n = min(hi, F) - lo
            found.append((dn.at[pl.ds(pl.multiple_of(h * F + lo, 16), n)], dst.at[pl.ds(lo, n)]))
        if hi > F:
            s = max(lo, F)
            n = hi - s
            found.append(
                (dn.at[pl.ds(pl.multiple_of(2 * F + h * rem + s - F, 16), n)], dst.at[pl.ds(s, n)])
            )
        return found

    def slot(a, zz, yy):
        if a < tiles:
            return gvb.at[a, zz, yy]
        if a < DN:
            return gtb.at[zz, yy]
        return dnb.at[zz, yy, pl.ds((a - DN) * dn_rows, dn_rows)]

    def fetch(k, src, dst):
        pltpu.make_async_copy(src, dst, loc_sem.at[k]).start()

    def ready(k, whole):
        pltpu.make_async_copy(whole, whole, loc_sem.at[k]).wait()

    GS, MO, TAILS, GV, DOWN = range(5)
    if packed:
        fetch(GS, gp, gsb.at[z, y])
    else:
        fetch(GS, gp, gsb.at[z, y, :, pl.ds(0, C)])
        fetch(GS, sp_, gsb.at[z, y, :, pl.ds(C, C)])
    fetch(MO, mo, mob.at[z, y])
    T = tails.shape[2]
    if packed:
        fetch(TAILS, gt, tails.at[0])
        fetch(TAILS, vt, tails.at[1])
    else:
        fetch(TAILS, gt.at[:, pl.ds(2 * F, T)], tails.at[0])
        fetch(TAILS, vt.at[:, pl.ds(2 * F, T)], tails.at[1])
    for a in range(tiles):
        for src, dst in parts(a, q, z, y):
            fetch(GV, src, dst)
    for a in range(DN, DN + dn_pieces):
        for src, dst in parts(a, q, z, y):
            fetch(DOWN, src, dst)

    barrier = pltpu.get_barrier_semaphore()
    peers = [zpeer(d) for d in range(1, nz)] + [ypeer(e) for e in range(1, ny)]
    peers += [tpeer(d, e) for d in range(nx) for e in range(2) if d + e]
    for p in peers:
        pl.semaphore_signal(barrier, inc=1, device_id=p, device_id_type=MESH)

    ready(TAILS, tails)
    for h in range(2):
        for k in range(2):
            mixed[h, :, k * (MW // 2):k * (MW // 2) + rem] = tails[k, :, h * rem:(h + 1) * rem]
    for k in range(2):
        part = tails[k].astype(F32)
        part = jnp.where(q == 0, part[:, :rem], part[:, rem:2 * rem]).astype(BF16)
        gtb[z, y, :, k * (MW // 2):k * (MW // 2) + rem] = part
    ready(GS, gsb.at[z, y])
    ready(MO, mob.at[z, y])
    pl.semaphore_wait(barrier, len(peers))

    def issue_z(a, d):
        for src, dst in parts(a, zsrc(d) % 2, z, y):
            remote(src, dst, common(family(a) + "_z"), z_sem(a, d), zpeer(d)).start()

    def z_sem(a, d):
        return gvr.at[a, d] if a < DN else dnr.at[a - DN, d]

    def y_sem(a, d, e):
        return gvy.at[a, e] if a < DN else dnr.at[dn_pieces + e - 1, d]

    def family(a):
        return "gv" if a < tiles else "gt" if a < DN else "dn"

    def issue_y(a):
        for e in range(1, ny):
            send(family(a) + "_y", slot(a, z, y), slot(a, z, y), y_sem(a, 0, e), ypeer(e))

    def relay(a, k):
        d, zz = source(k)
        arrived(slot(a, zz, y), z_sem(a, d))
        for e in range(1, ny):
            send(family(a) + "_y", slot(a, zz, y), slot(a, zz, y), y_sem(a, d, e), ypeer(e))

    bits = [1 << k for k in reversed(range((nz - 1).bit_length()))]

    def spread(kind, buf, d, rsem):
        src = zsrc(d)
        for bit in bits:
            if d == 0 or bit < (d & -d):
                send(kind, buf(src), buf(src), rsem.at[d | bit], zpeer(bit))

    def issue_far(a, what):
        if nz != 4:
            for d in range(2, nz):
                if (what == "n") == (d == 2) and what != "w" and (what != "m" or d > 2):
                    issue_z(a, d)
            return
        if what in "mw":
            pl.when(inner == (1 if what == "m" else 0))(lambda: issue_z(a, 3))
            return
        row = 2 - z // 2 if what == "n" else 3 - 3 * (z // 2)
        d = 2 + inner if what == "n" else 3 - inner
        for src, dst in parts(a, row % 2, z, y):
            remote(src, dst, common(family(a) + "_z"), z_sem(a, d), (row * ny + y, t)).start()

    def steps(plan):
        for what, piece, d in plan:
            if piece < TILES and piece >= tiles:
                continue
            a = piece if piece < TILES else piece - TILES + tiles
            if what == "o":
                issue_y(a)
            elif what in "nemw":
                issue_far(a, what)
            for dd in range(1, nz):
                if dd == d or (d == 3 and dd > 3):
                    (relay if what == "r" else issue_z)(a, dd)

    def gs_block(src):
        return gsb.at[src, y]

    def mo_block(src):
        return mob.at[src]

    spread("gs_z", gs_block, 0, gzr)
    for e in range(1, ny):
        send("mo_y", mob.at[z, y], mob.at[z, y], common(f"mo_y{e}r"), ypeer(e))
    for e in range(1, ny):
        send("gs_y", gsb.at[z, y], gsb.at[z, y], common(f"gs_y{e}r"), ypeer(e))
    ready(GV, gvb.at[:, z, y])
    steps(PLAN_Y0)
    steps(PLAN_FIRST)

    xin[x, c] = normalize(tok[...].astype(F32)).astype(BF16)
    s1 = [tsem() for _ in range(nx)]
    for d in range(1, nx):
        send("xin_x", xin.at[x, c], xin.at[x, c], s1[d], xpeer(d))
    send("xin_c", xin.at[x, c], xin.at[x, c], common("xin_cr"), cpeer)

    with scope("mo_y"):
        for e in range(1, ny):
            arrived(mob.at[z, ysrc(e)], common(f"mo_y{e}r"))
    spread("mo_z", mo_block, 0, mzr)
    steps(PLAN_M0)
    for d in range(1, nz):
        with scope(f"relay_gs{d}"):
            arrived(gs_block(zsrc(d)), gzr.at[d])
            spread("gs_z", gs_block, d, gzr)
            for e in range(1, ny):
                send("gs_y", gs_block(zsrc(d)), gs_block(zsrc(d)), common(f"gs_y{e}r"), ypeer(e))
    steps(PLAN_M)
    for d in range(1, nz):
        with scope(f"relay_mo{d}"):
            arrived(mo_block(zsrc(d)), mzr.at[d])
            spread("mo_z", mo_block, d, mzr)
    with scope("first_z"):
        steps(PLAN_0)
    ready(DOWN, dnb.at[z, y])
    steps(PLAN_Y)
    with scope("xin"):
        for d in range(1, nx):
            arrived(xin.at[xsrc(d), c], s1[d])
            send("xin_c", xin.at[xsrc(d), c], xin.at[xsrc(d), c], common("xin_cr"), cpeer)
        arrived(xin.at[:, 1 - c], common("xin_cr"))
    with scope("complete_gs"):
        for e in range(1, ny):
            arrived(gsb.at[:, ysrc(e)], common(f"gs_y{e}r"))

    with scope("mix_in"):
        pre = jnp.dot(xin[...].reshape(seq, D), gsb[...].reshape(D, 2 * C), preferred_element_type=F32)
        branch_signal = jax.nn.gelu(pre[:, C:])
        total = jnp.sum(branch_signal, axis=1, keepdims=True)
        square = jnp.sum(branch_signal * branch_signal, axis=1, keepdims=True)
        lane = lax.broadcasted_iota(jnp.int32, (seq, LANES), 1)
        stat[0] = jnp.where(lane == 0, total, square).T[:8]
    others = [(d, e) for d in range(nx) for e in range(2) if d + e]
    sx = {}
    for d, e in others:
        sx[d, e] = tsem()
        send("stat", stat.at[0], stat.at[2 * d + e], sx[d, e], tpeer(d, e))
    branch_gate = jax.nn.gelu(pre[:, :C])
    with scope("stats"):
        summed = stat[0]
        for d, e in others:
            arrived(stat.at[2 * d + e], sx[d, e])
            summed = summed + stat[2 * d + e]
    with scope("mix_out"):
        back = summed.T
        row_mean = back[:, 0:1] / MIX_WIDTH
        spread = back[:, 1:2] / MIX_WIDTH - row_mean * row_mean
        spatial_input = (
            (branch_signal - row_mean) * lax.rsqrt(spread + EPSILON) * wide(sgain)
        ).astype(BF16)
        rows_i = lax.broadcasted_iota(jnp.int32, (BLOCK, BLOCK), 0) // SEGMENT
        cols_i = lax.broadcasted_iota(jnp.int32, (BLOCK, BLOCK), 1) // SEGMENT
        own = spatial[t * C // HEAD_SIZE]
        own = jnp.where(cols_i <= rows_i, own, jnp.zeros_like(own))
        gated = jnp.concatenate(
            [
                branch_gate[b * BLOCK:(b + 1) * BLOCK]
                * jnp.dot(own, spatial_input[b * BLOCK:(b + 1) * BLOCK], preferred_element_type=F32)
                for b in range(seq // BLOCK)
            ],
            axis=0,
        ).astype(BF16)
        for k in range(nz * ny):
            part = jnp.dot(gated, mob[k // ny, k % ny], preferred_element_type=F32).astype(BF16)
            for b in range(nx * 2):
                pm[b % 2, b // 2, :, k * cw:(k + 1) * cw] = part[b * R:(b + 1) * R]
    sc = tsem()
    send("pm", pm.at[1 - c], prc, sc, cpeer)
    with scope("mix_core"):
        arrived(prc, sc)
    for b in range(nx):
        abm[b] = (pm[c, b].astype(F32) + prc[b].astype(F32)).astype(BF16)
    sx = [tsem() for _ in range(nx)]
    for d in range(1, nx):
        send("abm", abm.at[lax.rem(x + d, nx)], pxr.at[d - 1], sx[d], xpeer(d))
    with scope("relay_gv0"):
        steps(PLAN_A)
    with scope("mix_x"):
        for d in range(1, nx):
            arrived(pxr.at[d - 1], sx[d])
    with scope("mid"):
        mix_out = pm[c, x].astype(F32) + prc[x].astype(F32)
        for d in range(1, nx):
            mix_out = mix_out + pxr[d - 1].astype(F32)
        mid[...] = (
            normalize(RESIDUAL_SCALE * tok[...].astype(F32) + mix_out) * wide(mgain)
        ).astype(BF16)
        hin[q, x, c] = normalize(mid[...].astype(F32)).astype(BF16)

    sp = tsem()
    send("hin_z", hin.at[q, x, c], hin.at[q, x, c], sp, ppeer)
    sx = [[tsem() for _ in range(nx)] for _ in range(2)]

    def rows_out(k, s):
        for d in range(1, nx):
            send("hin_x", hin.at[s, x, c], hin.at[s, x, c], sx[k][d], xpeer(d))
        send("hin_c", hin.at[s, x, c], hin.at[s, x, c], common("hin_cr"), cpeer)

    def rows_over(k, s):
        for d in range(1, nx):
            arrived(hin.at[s, xsrc(d), c], sx[k][d])
            send("hin_c", hin.at[s, xsrc(d), c], hin.at[s, xsrc(d), c], common("hin_cr"), cpeer)

    rows_out(0, q)
    with scope("relay_b"):
        steps(PLAN_B)
    with scope("rows_x0"):
        rows_over(0, q)
    with scope("relay_c"):
        steps(PLAN_C)
    with scope("pair_rows"):
        arrived(hin.at[1 - q, x, c], sp)
    rows_out(1, 1 - q)
    with scope("relay_d"):
        steps(PLAN_D)
    with scope("rows_x1"):
        rows_over(1, 1 - q)
    with scope("rows_core"):
        arrived(hin.at[:, :, 1 - c], common("hin_cr"))
    def gate_value(a):
        lhs_rows = (hin[s].reshape(seq, D) for s in range(2))
        if a < tiles:
            weights = gvb[a].reshape(D, 2 * LANES)
            tap = taps[:, pl.ds(pl.multiple_of(q * F + a * LANES, LANES), LANES)].astype(F32)
            n, at = LANES, LANES
        else:
            weights = gtb[...].reshape(D, MW)
            tap = taps[:, 2 * F:2 * F + 2 * rem].astype(F32)
            tap = jnp.where(q == 0, tap[:, :rem], tap[:, rem:])
            n, at = rem, MW // 2
        for s, lhs in enumerate(lhs_rows):
            both = jnp.dot(lhs, weights, preferred_element_type=F32)
            gate, value = both[:, :n], both[:, at:at + n]
            row = lax.broadcasted_iota(jnp.int32, gate.shape, 0)
            one = jnp.where(row >= 1, pltpu.roll(gate, 1, 0), 0.0)
            two = jnp.where(row >= 2, pltpu.roll(gate, 2, 0), 0.0)
            conv = tap[0:1] * two + tap[1:2] * one + tap[2:3] * gate
            hid[s, :, a * LANES:a * LANES + n] = (jax.nn.silu(conv) * value).astype(BF16)

    for a in range(DN):
        with scope(f"complete_gv{a}"):
            for e in range(1, ny):
                whole = gvb.at[a, :, ysrc(e)] if a < tiles else gtb.at[:, ysrc(e)]
                arrived(whole, gvy.at[a, e])
        with scope(f"gate_value{a}"):
            gate_value(a)
        with scope("relay_e"):
            steps(PLAN_E.get(a if a < tiles else TILES, ()))

    groups = sorted(
        ((i, g) for i in range(nz) for g in range(len(subs))),
        key=lambda j: (j[0] >= nz // 2, j[1] > 0 and j[0] >= nz // 2, j),
    )
    sc = {j: [tsem() for _ in range(2)] for j in groups}
    sx = {j: [[tsem() for _ in range(nx)] for _ in range(2)] for j in groups}
    turns = (1 - q, q)
    split = len(subs) > 1

    def down(item):
        (i, g), k = item
        s, zz = turns[k], source(i)[1]
        for n, e in enumerate(subs[g]):
            yy = lax.rem(y + e, ny) if split else e
            part = jnp.dot(hid[s], dnb[zz, yy], preferred_element_type=F32).astype(BF16)
            for b in range(nx * 2):
                pb[b % 2, i, g, s, b // 2, :, n * cw:(n + 1) * cw] = part[b * R:(b + 1) * R]
        send("pb", pb.at[1 - c, i, g, s], rb.at[i, g, s], sc[i, g][k], cpeer)
        crossed.append(item)

    def over_x(item):
        (i, g), k = item
        s = turns[k]
        arrived(rb.at[i, g, s], sc[i, g][k])
        for b in range(nx):
            ab[i, g, s, b] = (pb[c, i, g, s, b].astype(F32) + rb[i, g, s, b].astype(F32)).astype(BF16)
        for d in range(1, nx):
            send("ab", ab.at[i, g, s, lax.rem(x + d, nx)], xr.at[i, g, d - 1, s], sx[i, g][k][d], xpeer(d))

    def over_z(item):
        (i, g), k = item
        s, zz = turns[k], source(i)[1]
        gg = lax.rem(y + subs[g][0], ny) if split else 0
        for d in range(1, nx):
            arrived(xr.at[i, g, d - 1, s], sx[i, g][k][d])
        acc = ab[i, g, s, x].astype(F32)
        for d in range(1, nx):
            acc = acc + xr[i, g, d - 1, s].astype(F32)
        zb[zz, gg, s] = acc.astype(BF16)
        if k == 0:
            send("zb", zb.at[zz, gg, s], zr.at[zz, gg], common("zbr"), ppeer)

    crossed, summed_up = [], []
    def flush(keep_x, keep_z):
        while len(crossed) > keep_x:
            j = crossed.pop(0)
            over_x(j)
            summed_up.append(j)
        while len(summed_up) > keep_z:
            over_z(summed_up.pop(0))

    def complete_dn(j):
        i, g = j
        with scope(f"complete_dn{i}{g}"):
            for e in range(1, ny):
                if (split and e in subs[g]) or not split:
                    b = ny - e if split else e
                    d, zz = source(i)
                    arrived(dnb.at[zz, ysrc(b)], dnr.at[dn_pieces + b - 1, d])

    for j in groups:
        complete_dn(j)
        with scope(f"down{j[0]}{j[1]}"):
            down((j, 0))
            down((j, 1))
        with scope(f"relay_h{j[0]}"):
            steps(PLAN_H.get(j, ()) if split else PLAN_H.get((j[0], 0), ()) + PLAN_H.get((j[0], 1), ()))
        with scope(f"flush{j[0]}{j[1]}"):
            flush(KEEP_X, KEEP_Z)
    with scope("tail_x"):
        flush(0, 0)
    with scope("tail_z"):
        arrived(zr, common("zbr"))
    with scope("final"):
        ffn_out = jnp.concatenate(
            [zb[zz, gg, q].astype(F32) + zr[zz, gg].astype(F32) for zz in range(nz) for gg in range(len(subs))],
            axis=1,
        )
        out[...] = (
            normalize(RESIDUAL_SCALE * mid[...].astype(F32) + ffn_out) * wide(ogain)
        ).astype(BF16)
    with scope("drain_end"):
        sent("gs_z", gsb.at[pl.ds(0, nz - 1), y])
        sent("mo_z", mob.at[pl.ds(0, nz - 1)])
        far = pl.ds(0, nz - 1)
        sent("gv_z", gvb.at[:, far, y])
        sent("gt_z", gtb.at[far, y])
        sent("dn_z", dnb.at[far, y])
        over_y = pl.ds(0, ny - 1)
        sent("mo_y", mob.at[z, over_y])
        sent("gs_y", gsb.at[:, over_y])
        sent("gv_y", gvb.at[:, :, over_y])
        sent("gt_y", gtb.at[:, over_y])
        sent("dn_y", dnb.at[:, over_y])
        sent("xin_x", xin.at[pl.ds(0, nx - 1), 0])
        sent("xin_c", xin.at[:, c])
        sent("stat", stat.at[pl.ds(0, 2 * nx - 1)])
        sent("pm", prc)
        sent("abm", pxr)
        sent("hin_z", hin.at[q, x, c])
        sent("hin_x", hin.at[:, pl.ds(0, nx - 1), c])
        sent("hin_c", hin.at[:, :, c])
        sent("pb", rb)
        sent("ab", xr)
        sent("zb", zr)


def shards(nf, nt, ny, tokens, gate_proj, signal_proj, spatial, signal_gain, mixer_out, mixer_gain, ffn_gate, ffn_value, conv_taps, ffn_down, output_gain):
    nz = nf // ny
    nx = nt // 2
    R, D = tokens.shape
    K, C = gate_proj.shape
    H = ffn_gate.shape[1]
    full = H // (2 * LANES) * LANES
    rem = H // 2 - full
    W = full + rem
    MW = -(-2 * rem // LANES) * LANES
    cw = mixer_out.shape[1]
    seq = nx * 2 * R
    subs = [(e,) for e in range(ny)] if cw % LANES == 0 else [tuple(range(ny))]
    gw = cw * len(subs[0])
    ns = len(subs)
    dn_pieces = DN_PIECES
    packed = bool(C % LANES or (2 * rem) % LANES)
    if packed:
        gp = jnp.concatenate([gate_proj, signal_proj], axis=1)
        gt, vt = ffn_gate[:, 2 * full:], ffn_value[:, 2 * full:]
    else:
        gp, gt, vt = gate_proj, ffn_gate, ffn_value

    vm = pltpu.VMEM
    dma = pltpu.SemaphoreType.DMA
    n_t = 6 * nx + 2 + nz * ns * (2 + 2 * nx)
    scratch = [
        vm((nz, ny, K, 2 * C), BF16),
        vm((nz, ny) + mixer_out.shape, BF16),
        vm((full // LANES, nz, ny, K, 2 * LANES), BF16),
        vm((nz, ny, K, MW), BF16),
        vm((nz, ny, W, cw), BF16),
        vm((2, K, 2 * rem), BF16),
        vm((2, K, MW), BF16),
        vm((nx, 2, R, D), BF16),
        vm((2 * nx, 8, seq), F32),
        vm((2, nx, R, D), BF16),
        vm((nx, R, D), BF16),
        vm((nx, R, D), BF16),
        vm((nx - 1, R, D), BF16),
        vm((R, D), BF16),
        vm((2, nx, 2, R, D), BF16),
        vm((2, seq, W), BF16),
        vm((2, nz, ns, 2, nx, R, gw), BF16),
        vm((nz, ns, 2, nx, R, gw), BF16),
        vm((nz, ns, 2, nx, R, gw), BF16),
        vm((nz, ns, nx - 1, 2, R, gw), BF16),
        vm((nz, ns, 2, R, gw), BF16),
        vm((nz, ns, R, gw), BF16),
        dma((5,)),
        dma((nz,)),
        dma((nz,)),
        dma((full // LANES + 1, nz)),
        dma((full // LANES + 1, ny)),
        dma((dn_pieces + ny - 1, nz)),
        dma((24 + 2 * (ny - 1),)),
        dma((n_t,)),
    ]
    here, there = pl.BlockSpec(memory_space=pltpu.VMEM), pl.BlockSpec(memory_space=pl.ANY)
    return pl.pallas_call(
        functools.partial(kernel, nz, ny, nx, full, rem, subs, packed, dn_pieces),
        out_shape=jax.ShapeDtypeStruct((R, D), BF16),
        in_specs=[here] + [there] * 8 + [here] * 5,
        out_specs=here,
        scratch_shapes=scratch,
        compiler_params=pltpu.CompilerParams(
            collective_id=0, has_side_effects=True, vmem_limit_bytes=67043328
        ),
    )(
        tokens, gp, signal_proj, mixer_out, ffn_gate, ffn_value, gt, vt, ffn_down, spatial,
        signal_gain, mixer_gain, conv_taps, output_gain,
    )


def solution(mesh):
    nf, nt = mesh.shape["fs"], mesh.shape["tp"]
    ny = 2 ** (int(math.log2(nf // 2)) // 2)
    in_specs = (
        P(("fs", "tp"), None),
        P("fs", "tp"),
        P("fs", "tp"),
        P(),
        P("tp"),
        P("tp", "fs"),
        P(),
        P("fs", "tp"),
        P("fs", "tp"),
        P(None, "tp"),
        P("tp", "fs"),
        P(),
    )
    return jax.shard_map(
        functools.partial(shards, nf, nt, ny),
        mesh=mesh,
        in_specs=in_specs,
        out_specs=P(("fs", "tp"), None),
        check_vma=False,
    )
```
